32 devices in a mesh: sp: 8 (over z, x), tp: 4 (over y, core).
Axes of the slice: x: 2, y: 2, z: 4, core: 2. Of those that a mesh axis runs over, the one named last changes fastest.
Arguments:
- layer_grad: bfloat16 [2048, 2048], P('sp', 'tp'), may hold values from -6 to 6
- routes: int32 [2048, 2], P('sp'), may hold values from 0 to 7, all different within a row; in each aligned block of 256 rows (0 to 255, 256 to 511, ...) at most 96 rows name the same one
- route_weights: float32 [2048, 2], P('sp'), may hold values from 0.1 to 0.9
- expert_in: bfloat16 [8, 768, 2048], P('sp', None, 'tp'), may hold values from -50 to 50
- w_gate: bfloat16 [8, 2048, 2048], P('sp', None, 'tp'), may hold values from -0.125 to 0.125
- w_up: bfloat16 [8, 2048, 2048], P('sp', None, 'tp'), may hold values from -0.125 to 0.125
- w_down: bfloat16 [8, 2048, 2048], P('sp', 'tp'), may hold values from -0.125 to 0.125
- conv_in: bfloat16 [2048, 512], P('sp', 'tp'), may hold values from -6 to 6
- c_gate: bfloat16 [2048, 512], P('sp', 'tp'), may hold values from -6 to 6
- b_gate: bfloat16 [2048, 512], P('sp', 'tp'), may hold values from -1.5 to 1.5
- conv_out: bfloat16 [2048, 512], P('sp', 'tp'), may hold values from -1.5 to 1.5
- taps: bfloat16 [3, 512], P(None, 'tp'), may hold values from -3.5 to 3.5
- w_out: bfloat16 [512, 2048], P('tp'), may hold values from -0.25 to 0.25
Outputs:
- grad_w_gate: bfloat16 [8, 2048, 2048], P('sp', None, 'tp')
- grad_w_up: bfloat16 [8, 2048, 2048], P('sp', None, 'tp')
- grad_w_down: bfloat16 [8, 2048, 2048], P('sp', 'tp')
- grad_routed: bfloat16 [2048, 2048], P('sp', 'tp')
- grad_out_proj: float32 [512, 2048], P('tp', 'sp')
- grad_conv_in: bfloat16 [2048, 512], P('sp', 'tp')
- grad_c_gate: bfloat16 [2048, 512], P('sp', 'tp')
- grad_b_gate: bfloat16 [2048, 512], P('sp', 'tp')
The draws below stay inside these ranges and needn't reach their ends.
Inputs may be any that keep to these rules, and one draw needn't show every extreme that they name: `routes`: each token names 2 different experts. Among the tokens of one block of 256, no expert is named more than 96 times, a bound that some block reaches.
All inputs are finite; a program needn't handle non-finite values.
Results may differ from the reference program's by a relative error of at most 0.019.
Values may be sent and summed in bfloat16 or wider, within the bound.
A program may use at most 64 MiB of HBM per device.

```python
import math
import jax
import jax.numpy as jnp
import numpy as np
from jax import lax

D = 2048
FF = 2048
CW = 512
TAPS = 3
TOP = 2
TOK_DEV = 256
TOKENS = 2048
EXPERTS = 8
CAP = 96
ROWS = 768
N_SP = 8
N_TP = 4


def draw_expert_in(key, part):
    base_key = jax.random.fold_in(key, 7)
    scale_key, value_key = jax.random.split(base_key)
    row_scale = jnp.exp(jax.random.uniform(scale_key, (EXPERTS, ROWS, 1), jnp.float32, math.log(0.3), math.log(3.0)))
    values = jnp.clip(jax.random.normal(value_key, (EXPERTS, ROWS, D), jnp.float32), -5.0, 5.0)
    return (values * row_scale).astype(jnp.bfloat16)


def strengthened(values, stream_key, source, target, shards_of, factor):
    owner, partner = [(jnp.arange(values.shape[axis_at]) // (values.shape[axis_at] // shards_of)).reshape([-1 if axis == axis_at else 1 for axis in range(values.ndim)]) for axis_at in (source, target)]
    chosen = jax.random.permutation(stream_key, shards_of)[partner]
    strong = (owner == chosen) | (owner == (partner + shards_of // 2) % shards_of)
    return jnp.where(strong, factor * values, values)


def block_levels(rng, shape, pieces, low, top_value):
    factor_of, own = 1.0, jax.random.fold_in(rng, 6)
    for axis_at, shards_of in pieces:
        steps = jnp.exp(jax.random.uniform(jax.random.fold_in(own, axis_at), (shards_of,), jnp.float32, low / len(pieces), top_value / len(pieces)))
        factor_of = factor_of * jnp.repeat(steps, shape[axis_at] // shards_of).reshape([-1 if axis == axis_at else 1 for axis in range(len(shape))])
    return factor_of


def shared_out(key, own, number, rows, count, top, reach, lean):
    sequence = jax.random.permutation(key, count)
    packed, ordinary = shares(count, rows * top, reach, lean, True), shares(count, rows * top, reach, lean, False)
    places = jnp.arange(count)

    def named(lengths, rotation):
        used = int((lengths > 0).sum())
        fixed = max(1, used // 4)
        passed = fixed + (places - fixed + rotation * (used - fixed)) % max(1, count - fixed)
        return jnp.zeros((count,), jnp.int32).at[sequence[jnp.where(places < fixed, places, passed)]].set(jnp.asarray(lengths, jnp.int32))

    lengths = jnp.where(number % 4 == 0, named(packed, number // 4), named(ordinary, number - number // 4 - 1))
    mixed = jax.random.permutation(jax.random.fold_in(own, 3), count)
    giver, sink = mixed[0:count // 2 * 2:2], mixed[1:count // 2 * 2:2]
    margin = jnp.minimum(lengths[giver] - 1, reach - lengths[sink]) // 2
    margin = jnp.where((giver == sequence[0]) | (sink == sequence[0]) | (lengths[sink] == 0), 0, jnp.maximum(margin, 0))
    passed = jax.random.randint(jax.random.fold_in(own, 4), (count // 2,), 0, 1 << 20) % (margin + 1)
    lengths = lengths.at[giver].add(-passed).at[sink].add(passed)
    members = jnp.searchsorted(jnp.cumsum(lengths), jnp.arange(rows * top), side="right").astype(jnp.int32)
    table = members.reshape(top, rows).T
    table = table[jax.random.permutation(jax.random.fold_in(own, 1), rows)]
    rotation = jax.random.randint(jax.random.fold_in(own, 2), (rows, 1), 0, top)
    return jnp.take_along_axis(table, (jnp.arange(top)[None, :] + rotation) % top, axis=1)


def shares(number_of, total, limit, skew, full):
    weights = [(1 << 20) // math.isqrt(grade ** skew) + 1 for grade in range(1, number_of + 1)]
    largest = limit if full else min(limit, max(-(-total // number_of), total * weights[0] // sum(weights)))
    least = 1 if total - largest >= number_of - 1 else 0
    counts, rest = [largest] + [least] * (number_of - 1), total - largest - least * (number_of - 1)
    while rest > 0:
        free = [i for i in range(1, number_of) if counts[i] < largest] or [i for i in range(1, number_of) if counts[i] < limit]
        pool, left = sum([weights[i] for i in free]), rest
        for i in free:
            addition = min(limit - counts[i], max(1, left * weights[i] // pool), rest)
            counts[i] = counts[i] + addition
            rest = rest - addition
    return np.array(counts)


def normal_values(key, extent, deviation, most, shards=(), held_as=jnp.bfloat16):
    loudness = block_levels(key, extent, shards, -0.22, 0.18) if shards else 1.0
    result = jax.random.normal(key, extent, jnp.float32) * deviation * loudness
    return jnp.minimum(jnp.maximum(result, -most), most).astype(held_as)


def noise_with(rng, dims, deviation, reach, shards, heavy, held_as=jnp.bfloat16):
    entries = deviation * jax.random.normal(rng, dims, jnp.float32)
    if shards:
        entries = entries * block_levels(rng, dims, shards, -0.22, 0.18)
    return jnp.clip(strengthened(entries, jax.random.fold_in(rng, 3), *heavy), -reach, reach).astype(held_as)


def setup_inputs(seed: int = 0) -> dict:
    key_of = jax.random.split(jax.random.key(seed), 14)
    layer_grad = noise_with(key_of[0], (TOKENS, D), 1.0, 6.0, ((0, 8), (1, 4)), (0, 1, 8, 2.0))
    routes_keys = jax.random.split(jax.random.fold_in(key_of[1], 1), TOKENS // TOK_DEV)
    routes_turns = jax.random.permutation(jax.random.fold_in(key_of[1], 3), TOKENS // TOK_DEV)
    routes = jax.vmap(lambda own, number: shared_out(jax.random.fold_in(key_of[1], 2), own, number, TOK_DEV, EXPERTS, TOP, CAP, 1))(routes_keys, routes_turns).reshape((TOKENS, TOP))
    route_weights = jnp.clip(0.1 + 0.79999997 * jax.random.uniform(key_of[2], (TOKENS, TOP), jnp.float32) ** block_levels(key_of[2], (TOKENS, TOP), ((0, 8),), -0.2, 0.2), 0.1, 0.9)
    expert_in = draw_expert_in(jax.random.fold_in(key_of[13], 71), 0)
    w_gate = normal_values(key_of[4], (EXPERTS, D, FF), D ** -0.5, 0.125, ((0, 8), (2, 4)))
    w_up = normal_values(key_of[5], (EXPERTS, D, FF), D ** -0.5, 0.125, ((0, 8), (2, 4)))
    w_down = normal_values(key_of[6], (EXPERTS, FF, D), FF ** -0.5, 0.125, ((0, 8), (1, 4)))
    conv_in = normal_values(key_of[7], (TOKENS, CW), 1.0, 6.0, ((0, 8), (1, 4)))
    c_gate = normal_values(key_of[8], (TOKENS, CW), 1.0, 6.0, ((0, 8), (1, 4)))
    b_gate = normal_values(key_of[9], (TOKENS, CW), 0.25, 1.5, ((0, 8), (1, 4)))
    conv_out = normal_values(key_of[10], (TOKENS, CW), 0.25, 1.5, ((0, 8), (1, 4)))
    taps = normal_values(key_of[11], (TAPS, CW), TAPS ** -0.5, 3.5, ((1, 4),))
    w_out = normal_values(key_of[12], (CW, D), CW ** -0.5, 0.25, ((0, 4),))
    return dict(layer_grad=layer_grad, routes=routes, route_weights=route_weights, expert_in=expert_in, w_gate=w_gate, w_up=w_up, w_down=w_down, conv_in=conv_in, c_gate=c_gate, b_gate=b_gate, conv_out=conv_out, taps=taps, w_out=w_out)


clamp_limit = 7.0
swish_alpha = 1.702


def slot_rows(routes):
    blocks = routes.reshape(N_SP, TOK_DEV * TOP)
    onehot = (blocks[:, :, None] == jnp.arange(EXPERTS, dtype=jnp.int32)[None, None, :]).astype(jnp.int32)
    slot_rank = jnp.sum((jnp.cumsum(onehot, axis=1) - 1) * onehot, axis=2).astype(jnp.int32)
    source = jnp.arange(N_SP, dtype=jnp.int32)[:, None]
    return (blocks * ROWS + source * CAP + slot_rank).reshape(-1).astype(jnp.int32)


def expert_grads(operands):
    expert_grad, saved_rows, gate_weight, up_weight, down_weight = operands
    gate_pre = jnp.dot(saved_rows, gate_weight, preferred_element_type=jnp.float32)
    up_pre = jnp.dot(saved_rows, up_weight, preferred_element_type=jnp.float32)
    gate_cut = jnp.minimum(gate_pre, clamp_limit)
    up_cut = jnp.clip(up_pre, -clamp_limit, clamp_limit)
    sigmoid_gate = jax.nn.sigmoid(swish_alpha * gate_cut)
    hidden = ((up_cut + 1.0) * gate_cut * sigmoid_gate).astype(jnp.bfloat16)
    act_grad = jnp.dot(expert_grad, down_weight.T, preferred_element_type=jnp.float32)
    grad_down = jnp.dot(hidden.T, expert_grad, preferred_element_type=jnp.float32).astype(jnp.bfloat16)
    slope = sigmoid_gate + swish_alpha * gate_cut * sigmoid_gate * (1.0 - sigmoid_gate)
    gate_grad = jnp.where(gate_pre < clamp_limit, act_grad * (up_cut + 1.0) * slope, 0.0).astype(jnp.bfloat16)
    up_grad = jnp.where(jnp.abs(up_pre) < clamp_limit, act_grad * gate_cut * sigmoid_gate, 0.0).astype(jnp.bfloat16)
    grad_gate = jnp.dot(saved_rows.T, gate_grad, preferred_element_type=jnp.float32).astype(jnp.bfloat16)
    grad_up = jnp.dot(saved_rows.T, up_grad, preferred_element_type=jnp.float32).astype(jnp.bfloat16)
    blocked_gate = gate_grad.astype(jnp.float32).reshape(ROWS, N_TP, FF // N_TP)
    blocked_up = up_grad.astype(jnp.float32).reshape(ROWS, N_TP, FF // N_TP)
    weight_gate = gate_weight.astype(jnp.float32).reshape(D, N_TP, FF // N_TP)
    weight_up = up_weight.astype(jnp.float32).reshape(D, N_TP, FF // N_TP)
    terms = jnp.einsum('rjf,djf->jrd', blocked_gate, weight_gate) + jnp.einsum('rjf,djf->jrd', blocked_up, weight_up)
    rounded = lax.optimization_barrier(terms.astype(jnp.bfloat16))
    input_grad = jnp.sum(rounded.astype(jnp.float32), axis=0).astype(jnp.bfloat16)
    return grad_gate, grad_up, grad_down, input_grad


def reference(layer_grad, routes, route_weights, expert_in, w_gate, w_up, w_down, conv_in, c_gate, b_gate, conv_out, taps, w_out):
    slot_index = slot_rows(routes)
    scaled = (route_weights[:, :, None] * layer_grad[:, None, :].astype(jnp.float32)).astype(jnp.bfloat16)
    scaled = scaled.reshape(TOKENS * TOP, D)
    expert_grad = jnp.zeros((EXPERTS * ROWS, D), jnp.bfloat16).at[slot_index].set(scaled).reshape(EXPERTS, ROWS, D)
    grad_gate, grad_up, grad_down, input_grad = lax.map(expert_grads, (expert_grad, expert_in, w_gate, w_up, w_down))
    picked = input_grad.reshape(EXPERTS * ROWS, D)[slot_index].reshape(TOKENS, TOP, D)
    grad_routed = jnp.sum(picked.astype(jnp.float32), axis=1).astype(jnp.bfloat16)
    mixer_grad = jnp.dot(layer_grad, w_out.T, preferred_element_type=jnp.float32)
    mixed = (b_gate.astype(jnp.float32) * conv_out.astype(jnp.float32)).astype(jnp.bfloat16)
    grad_out_proj = jnp.dot(mixed.T, layer_grad, preferred_element_type=jnp.float32)
    out_grad = mixer_grad * b_gate.astype(jnp.float32)
    padded = jnp.pad(out_grad, ((0, TAPS - 1), (0, 0)))
    tap_values = taps.astype(jnp.float32)
    conv_grad = jnp.zeros((TOKENS, CW), jnp.float32)
    for tap_index in range(TAPS):
        offset = TAPS - 1 - tap_index
        conv_grad = conv_grad + tap_values[tap_index] * padded[offset:offset + TOKENS]
    grad_conv_in = (conv_grad * c_gate.astype(jnp.float32)).astype(jnp.bfloat16)
    grad_c_gate = (conv_grad * conv_in.astype(jnp.float32)).astype(jnp.bfloat16)
    grad_b_gate = (mixer_grad * conv_out.astype(jnp.float32)).astype(jnp.bfloat16)
    return (grad_gate, grad_up, grad_down, grad_routed, grad_out_proj, grad_conv_in, grad_c_gate, grad_b_gate)
```

```python
import functools

import jax
import jax.numpy as jnp
from jax import lax
from jax.experimental import pallas as pl
from jax.experimental.pallas import tpu as pltpu
from jax.sharding import PartitionSpec as P

clamp_limit = 7.0
swish_alpha = 1.702


def passed_along(value, axis, steps):
    count = lax.axis_size(axis)
    leading, last = (max(0, -steps), min(count, count - steps))
    return lax.ppermute(value, axis, [(source, source + steps) for source in range(leading, last)])


def per_device(
    layer_grad,
    routes,
    route_weights,
    expert_in,
    w_gate,
    w_up,
    w_down,
    conv_in,
    c_gate,
    b_gate,
    conv_out,
    taps,
    w_out,
):
    sp_devices = lax.axis_size("sp")
    tok_rows = layer_grad.shape[0]
    top_count = routes.shape[1]
    capacity = expert_in.shape[1] // sp_devices
    full_grad = lax.all_gather(layer_grad, "tp", axis=1, tiled=True)
    flat_routes = routes.reshape(-1)
    onehot = (flat_routes[:, None] == jnp.arange(sp_devices, dtype=jnp.int32)[None, :]).astype(
        jnp.int32
    )
    slot_rank = jnp.sum((jnp.cumsum(onehot, axis=0) - 1) * onehot, axis=1)
    slot_index = flat_routes * capacity + slot_rank
    weights = route_weights[:, :, None]
    scaled = (weights * layer_grad[:, None, :].astype(jnp.float32)).astype(jnp.bfloat16)
    scaled = scaled.reshape(tok_rows * top_count, -1)
    buffer = (
        jnp.zeros((sp_devices * capacity, scaled.shape[1]), jnp.bfloat16).at[slot_index].set(scaled)
    )
    arrived = lax.all_to_all(
        buffer.reshape(sp_devices, capacity, -1), "sp", split_axis=0, concat_axis=0, tiled=True
    )
    expert_grad, saved_rows = (
        lax.all_gather(arrived.reshape(sp_devices * capacity, -1), "tp", axis=1, tiled=True),
        lax.all_gather(expert_in[0], "tp", axis=1, tiled=True),
    )
    gate_weight = w_gate[0]
    up_weight = w_up[0]
    down_weight = w_down[0]
    gate_pre = jnp.dot(saved_rows, gate_weight, preferred_element_type=jnp.float32)
    up_pre = jnp.dot(saved_rows, up_weight, preferred_element_type=jnp.float32)
    gate_cut = jnp.minimum(gate_pre, clamp_limit)
    up_cut = jnp.clip(up_pre, -clamp_limit, clamp_limit)
    sigmoid_gate = jax.nn.sigmoid(swish_alpha * gate_cut)
    hidden = ((up_cut + 1.0) * gate_cut * sigmoid_gate).astype(jnp.bfloat16)
    act_grad = jnp.einsum("rd,fd->rf", expert_grad, down_weight, preferred_element_type=jnp.float32)
    grad_down = jnp.einsum(
        "rf,rd->fd", hidden, expert_grad, preferred_element_type=jnp.float32
    ).astype(jnp.bfloat16)
    slope = sigmoid_gate + swish_alpha * gate_cut * sigmoid_gate * (1.0 - sigmoid_gate)
    gate_grad = jnp.where(gate_pre < clamp_limit, act_grad * (up_cut + 1.0) * slope, 0.0).astype(
        jnp.bfloat16
    )
    up_grad = jnp.where(
        jnp.abs(up_pre) < clamp_limit, act_grad * gate_cut * sigmoid_gate, 0.0
    ).astype(jnp.bfloat16)
    grad_gate = jnp.einsum(
        "rd,rf->df", saved_rows, gate_grad, preferred_element_type=jnp.float32
    ).astype(jnp.bfloat16)
    grad_up = jnp.einsum(
        "rd,rf->df", saved_rows, up_grad, preferred_element_type=jnp.float32
    ).astype(jnp.bfloat16)
    partial_value = jnp.einsum(
        "rf,df->rd", gate_grad, gate_weight, preferred_element_type=jnp.float32
    )
    partial_value = partial_value + jnp.einsum(
        "rf,df->rd", up_grad, up_weight, preferred_element_type=jnp.float32
    )
    rounded_terms = partial_value.astype(jnp.bfloat16)
    reduced = (
        lax.psum_scatter(rounded_terms, "tp", scatter_dimension=1, tiled=True)
        .astype(jnp.float32)
        .astype(jnp.bfloat16)
    )
    returned = lax.all_to_all(
        reduced.reshape(sp_devices, capacity, -1), "sp", split_axis=0, concat_axis=0, tiled=True
    )
    returned = returned.reshape(sp_devices * capacity, -1)
    picked = returned[slot_index]
    picked = picked.reshape(tok_rows, top_count, -1)
    grad_routed = jnp.sum(picked.astype(jnp.float32), axis=1).astype(jnp.bfloat16)
    mixer_grad = jnp.einsum("td,cd->tc", full_grad, w_out, preferred_element_type=jnp.float32)
    mixed = (b_gate.astype(jnp.float32) * conv_out.astype(jnp.float32)).astype(jnp.bfloat16)
    projected = lax.psum_scatter(
        jnp.einsum("td,tc->dc", full_grad, mixed, preferred_element_type=jnp.float32),
        "sp",
        scatter_dimension=0,
        tiled=True,
    )
    grad_out_proj = projected.T
    out_grad = mixer_grad * b_gate.astype(jnp.float32)
    tap_reach = taps.shape[0] - 1
    following = passed_along(out_grad[:tap_reach], "sp", -1)
    extended = jnp.concatenate([out_grad, following], axis=0)
    tap_values = taps.astype(jnp.float32)
    conv_grad = jnp.zeros_like(out_grad)
    for tap_index in range(tap_reach + 1):
        offset = tap_reach - tap_index
        conv_grad = conv_grad + tap_values[tap_index] * extended[offset : offset + tok_rows]
    grad_conv_in = (conv_grad * c_gate.astype(jnp.float32)).astype(jnp.bfloat16)
    grad_c_gate = (conv_grad * conv_in.astype(jnp.float32)).astype(jnp.bfloat16)
    grad_b_gate = (mixer_grad * conv_out.astype(jnp.float32)).astype(jnp.bfloat16)
    return (
        grad_gate[None],
        grad_up[None],
        grad_down[None],
        grad_routed,
        grad_out_proj,
        grad_conv_in,
        grad_c_gate,
        grad_b_gate,
    )


MESH = pl.DeviceIdType.MESH
bf16 = jnp.bfloat16
f32 = jnp.float32


def dot_nn(a, b):
    return jnp.dot(a, b, preferred_element_type=f32)


def dot_nt(a, b):
    return lax.dot_general(a, b, (((1,), (1,)), ((), ())), preferred_element_type=f32)


def dot_tn(a, b):
    return lax.dot_general(a, b, (((0,), (0,)), ((), ())), preferred_element_type=f32)


EXCHANGED = ("mirror",)
FIRST_SAVED = ("own", "mirror", "beyond")


def fused_kernel(
    n_sp,
    lg_hbm,
    rt_hbm,
    wt_hbm,
    ein_hbm,
    wg_hbm,
    wu_hbm,
    wd_hbm,
    ci_hbm,
    cg_hbm,
    bg_hbm,
    co_hbm,
    taps_hbm,
    wo_hbm,
    gg_v,
    gu_v,
    gd_v,
    sel,
    ret,
    gop_ref,
    gci_ref,
    gcg_ref,
    gbg_ref,
    wg,
    wu,
    wd,
    wg_t,
    wu_t,
    wd_t,
    wo,
    fg,
    saved,
    saved_t,
    eg,
    disp,
    disp_far,
    row_scale,
    proj,
    proj_x,
    proj_xr,
    proj_n,
    proj_nr,
    proj_a,
    proj_ar,
    ext,
    halo,
    hid,
    hidden_t,
    fac_g,
    fac_u,
    ggrad,
    ugrad,
    terms,
    px,
    ysend,
    yrecv,
    red,
    rt_ref,
    wt_ref,
    ci_ref,
    cg_ref,
    bg_ref,
    co_ref,
    taps_ref,
    load_s,
    lg_s,
    lg_r,
    ein_s,
    ein_r,
    disp_s,
    disp_r,
    far_s,
    far_r,
    egs_s,
    egs_r,
    swap_s,
    swap_r,
    proj_s,
    proj_r,
    halo_s,
    halo_r,
    d2d_s,
    d2d_r,
    y_s,
    y_r,
    ret_s,
    ret_r,
):
    sp = lax.axis_index("sp")
    tp = lax.axis_index("tp")
    core, chip = lax.rem(tp, 2), lax.div(tp, 2)
    partner = chip * 2 + (1 - core)
    across = (1 - chip) * 2 + core
    plane, side = lax.div(sp, 2), lax.rem(sp, 2)
    planes = n_sp // 2
    sibling = plane * 2 + (1 - side)
    near = plane + 1 - 2 * lax.rem(plane, 2)
    mirror = lax.rem(plane + 2, planes)
    beyond = lax.rem(near + 2, planes)
    rows, dcols = ein_hbm.shape
    cap = rows // n_sp
    pair = 2 * cap
    width = fg.shape[1]
    tokens = fg.shape[0]
    top = rt_hbm.shape[0]
    quads = {"own": plane, "near": near, "mirror": mirror, "beyond": beyond}
    index = {"own": 0, "near": 1, "mirror": 2, "beyond": 3}

    def cols(j):
        return pl.ds(pl.multiple_of(j * dcols, dcols), dcols)

    def block(b):
        return pl.ds(pl.multiple_of(b * cap, cap), cap)

    def pair_rows(q):
        return pl.ds(pl.multiple_of(q * pair, pair), pair)

    mine, other = cols(tp), cols(across)
    corner = cols((1 - chip) * 2 + (1 - core))

    def load(src, dst, n):
        copy = pltpu.make_async_copy(src, dst, load_s.at[n])
        copy.start()
        return copy

    def remote(src, dst, send, recv, to_sp, to_tp):
        return pltpu.make_async_remote_copy(
            src_ref=src,
            dst_ref=dst,
            send_sem=send,
            recv_sem=recv,
            device_id=(to_sp, to_tp),
            device_id_type=MESH,
        )

    barrier = pltpu.get_barrier_semaphore()
    pl.semaphore_signal(barrier, inc=1, device_id=(sp, partner), device_id_type=MESH)
    pl.semaphore_signal(barrier, inc=1, device_id=(sp, across), device_id_type=MESH)
    for i in range(1, n_sp):
        pl.semaphore_signal(
            barrier, inc=1, device_id=(lax.rem(sp + i, n_sp), tp), device_id_type=MESH
        )
    lg_load = load(lg_hbm, fg.at[:, mine], 0)
    ein_load = load(ein_hbm, saved.at[:, mine], 1)
    route_load = load(rt_hbm, rt_ref, 6)
    weight_load = load(wt_hbm, wt_ref, 7)
    mixer_loads = [
        load(bg_hbm, bg_ref, 8),
        load(co_hbm, co_ref, 9),
        load(ci_hbm, ci_ref, 10),
        load(cg_hbm, cg_ref, 11),
        load(taps_hbm, taps_ref, 12),
    ]
    wo_load = load(wo_hbm, wo, 2)
    wg_load = load(wg_hbm, wg, 3)
    wu_load = load(wu_hbm, wu, 4)
    wd_load = load(wd_hbm, wd, 5)
    pl.semaphore_wait(barrier, n_sp + 1)

    def send(copy):
        copy.start()
        return copy

    def sent(region, sem):
        remote(region, region, sem, sem, sp, partner).wait_send()

    def await_region(region, s_sem, r_sem):
        remote(region, region, s_sem, r_sem, sp, partner).wait_recv()

    def saved_across(name, sides=(0, 1)):
        i = index[name]
        for x in sides:
            sl = block(quads[name] * 2 + x)
            dst = saved.at[sl, mine]
            send(remote(ein_hbm.at[sl, :], dst, ein_s, ein_r.at[i], sp, across))

    def saved_relay(name):
        region, i = saved.at[pair_rows(quads[name]), other], index[name]
        await_region(region, ein_s, ein_r.at[i])
        send(remote(region, region, ein_s, ein_r.at[5 + i], sp, partner))

    def saved_arrive(name):
        region = saved.at[pair_rows(quads[name]), corner]
        await_region(region, ein_s, ein_r.at[5 + index[name]])

    def homes(name, sides=(0, 1)):
        return [sibling] if name == "own" else [quads[name] * 2 + x for x in sides]

    def rows_from(name):
        return block(sibling) if name == "own" else pair_rows(quads[name])

    send(remote(lg_hbm, fg.at[:, mine], lg_s, lg_r.at[0], sp, across))
    saved_across("mirror")
    saved_across("own")
    send(remote(lg_hbm, fg.at[:, mine], lg_s, lg_r.at[1], sp, partner))
    send(remote(ein_hbm, saved.at[:, mine], ein_s, ein_r.at[4], sp, partner))

    route_load.wait()
    weight_load.wait()
    expert_ids = lax.broadcasted_iota(jnp.int32, (n_sp, tokens), 0)
    named = jnp.zeros((n_sp, tokens), f32)
    weight = jnp.zeros((n_sp, tokens), f32)
    for k in range(top):
        hit = rt_ref[k : k + 1, :] == expert_ids
        named = jnp.where(hit, 1.0, named)
        weight = jnp.where(hit, wt_ref[k : k + 1, :], weight)
    earlier = (
        lax.broadcasted_iota(jnp.int32, (tokens, tokens), 0)
        < lax.broadcasted_iota(jnp.int32, (tokens, tokens), 1)
    )
    rank = dot_nn(named.astype(bf16), jnp.where(earlier, 1.0, 0.0).astype(bf16))
    rank = jnp.where(named > 0.0, rank, -1.0)
    slots = lax.broadcasted_iota(jnp.int32, (cap, tokens), 0).astype(f32)
    lg_load.wait()
    own_grad = fg[:, mine]
    for e in range(n_sp):
        chosen = slots == rank[e : e + 1, :]
        picks = jnp.where(chosen, 1.0, 0.0)
        row_weight = jnp.sum(jnp.where(chosen, weight[e : e + 1, :], 0.0), axis=1, keepdims=True)
        here = slice(e * cap, (e + 1) * cap)
        sel[here, :] = picks.astype(bf16)
        row_scale[here, :] = jnp.broadcast_to(row_weight, (cap, row_scale.shape[1]))
        disp[here, :] = (dot_nn(picks.astype(bf16), own_grad) * row_weight).astype(bf16)

    def dispatch(names):
        for name in names:
            for dest in homes(name):
                src, dst = disp.at[block(dest), :], eg.at[block(sp), mine]
                send(remote(src, dst, disp_s, disp_r.at[index[name]], dest, tp))

    def dispatch_far(names):
        for name in names:
            for dest in homes(name):
                src, dst = disp_far.at[block(dest), :], eg.at[block(sp), other]
                send(remote(src, dst, far_s, far_r.at[index[name]], dest, tp))

    def lg_relay():
        await_region(fg.at[:, other], lg_s, lg_r.at[0])
        send(remote(fg.at[:, other], fg.at[:, other], lg_s, lg_r.at[2], sp, partner))

    def select_across():
        far_grad = fg[:, other]
        for e in range(n_sp):
            here = slice(e * cap, (e + 1) * cap)
            disp_far[here, :] = (dot_nn(sel[here, :], far_grad) * row_scale[here, 0:1]).astype(bf16)

    def flip(src, dst):
        step = 512

        def part(j, carry):
            sl = pl.ds(pl.multiple_of(j * step, step), step)
            if src.shape[0] > src.shape[1]:
                dst[:, sl] = jnp.transpose(src[sl, :])
            else:
                dst[sl, :] = jnp.transpose(src[:, sl])
            return carry

        lax.fori_loop(0, width // step, part, 0)

    share = width // n_sp

    def mixer():
        wo_load.wait()
        for one in mixer_loads:
            one.wait()
        await_region(fg.at[:, cols(partner)], lg_s, lg_r.at[1])
        await_region(fg.at[:, corner], lg_s, lg_r.at[2])
        b_gate = bg_ref[...].astype(f32)
        conv_out = co_ref[...].astype(f32)
        mixer_grad = dot_nt(fg[...], wo[...])
        ext[0:tokens, :] = mixer_grad * b_gate
        gbg_ref[...] = (mixer_grad * conv_out).astype(bf16)
        before = lax.rem(sp + n_sp - 1, n_sp)
        halo_copy = send(remote(ext.at[0:8, :], halo, halo_s, halo_r, before, tp))
        mixed = (b_gate * conv_out).astype(bf16)
        for d in range(n_sp):
            proj[d % 2, d // 2] = dot_tn(mixed, fg[:, d * share : (d + 1) * share])
        proj_x[...] = proj[1 - side].astype(bf16)
        send(remote(proj_x, proj_xr, proj_s.at[0], proj_r.at[0], sibling, tp))
        return halo_copy

    def proj_near():
        await_region(proj_xr, proj_s.at[0], proj_r.at[0])
        for q in range(planes):
            proj[0, q] = proj[side, q] + proj_xr[q].astype(f32)
        proj_n[0] = proj[0, near].astype(bf16)
        proj_n[1] = proj[0, beyond].astype(bf16)
        send(remote(proj_n, proj_nr, proj_s.at[1], proj_r.at[1], near * 2 + side, tp))

    def proj_mirror():
        await_region(proj_nr, proj_s.at[1], proj_r.at[1])
        proj_a[...] = (proj[0, mirror] + proj_nr[1].astype(f32)).astype(bf16)
        send(remote(proj_a, proj_ar, proj_s.at[2], proj_r.at[2], mirror * 2 + side, tp))

    def proj_total():
        await_region(proj_ar, proj_s.at[2], proj_r.at[2])
        gop_ref[...] = proj[0, plane] + proj_nr[0].astype(f32) + proj_ar[...].astype(f32)

    def eg_mine(name):
        i, region = index[name], eg.at[pair_rows(quads[name]), mine]
        await_region(eg.at[rows_from(name), mine], disp_s, disp_r.at[i])
        if name in EXCHANGED:
            send(remote(region, region, swap_s, swap_r.at[EXCHANGED.index(name)], sp, across))
        send(remote(region, region, egs_s, egs_r.at[i], sp, partner))

    def eg_other(name):
        i, region = index[name], eg.at[pair_rows(quads[name]), other]
        if name in EXCHANGED:
            await_region(region, swap_s, swap_r.at[EXCHANGED.index(name)])
        else:
            await_region(eg.at[rows_from(name), other], far_s, far_r.at[i])
        send(remote(region, region, egs_s, egs_r.at[4 + i], sp, partner))

    def eg_arrive(name):
        sl, i = pair_rows(quads[name]), index[name]
        await_region(eg.at[sl, cols(partner)], egs_s, egs_r.at[i])
        await_region(eg.at[sl, corner], egs_s, egs_r.at[4 + i])

    def forward(name):
        sl = pair_rows(quads[name])
        x = saved[sl, :]
        gate_pre = dot_nn(x, wg[...])
        up_pre = dot_nn(x, wu[...])
        gate_cut = jnp.minimum(gate_pre, clamp_limit)
        up_cut = jnp.clip(up_pre, -clamp_limit, clamp_limit)
        sig = jax.nn.sigmoid(swish_alpha * gate_cut)
        base = gate_cut * sig
        slope = sig + swish_alpha * base * (1.0 - sig)
        hid[sl, :] = ((up_cut + 1.0) * base).astype(bf16)
        fac_g[sl, :] = jnp.where(gate_pre < clamp_limit, (up_cut + 1.0) * slope, 0.0)
        fac_u[sl, :] = jnp.where(jnp.abs(up_pre) < clamp_limit, base, 0.0)

    def backward(name):
        sl, i = pair_rows(quads[name]), index[name]
        act_grad = dot_nn(eg[sl, :], wd_t[...])
        g = (act_grad * fac_g[sl, :]).astype(bf16)
        u = (act_grad * fac_u[sl, :]).astype(bf16)
        ggrad[sl, :] = g
        ugrad[sl, :] = u

        def term(m):
            j = cols(m)
            terms[sl, j] = (dot_nn(g, wg_t[:, j]) + dot_nn(u, wu_t[:, j])).astype(bf16)

        for y in range(2):
            there = y * 2 + (1 - core)
            term(there)
            send(
                remote(
                    terms.at[sl, cols(there)],
                    px.at[sl, y * dcols : (y + 1) * dcols],
                    d2d_s,
                    d2d_r.at[i],
                    sp,
                    partner,
                )
            )
        for y in range(2):
            term(y * 2 + core)

    def pass_on(name):
        sl, i = pair_rows(quads[name]), index[name]
        await_region(px.at[sl, :], d2d_s, d2d_r.at[i])
        far = terms[sl, other].astype(f32) + px[sl, cols(1 - chip)].astype(f32)
        ysend[sl, :] = far.astype(bf16)
        send(remote(ysend.at[sl, :], yrecv.at[sl, :], y_s, y_r.at[i], sp, across))

    def add_up(name):
        sl, i = pair_rows(quads[name]), index[name]
        await_region(yrecv.at[sl, :], y_s, y_r.at[i])
        near_sum = terms[sl, mine].astype(f32) + px[sl, cols(chip)].astype(f32)
        red[sl, :] = (near_sum + yrecv[sl, :].astype(f32)).astype(bf16)
        if name == "own":
            ret[block(sp), :] = red[block(sp), :]

    def give(name, sides=(0, 1)):
        for dest in homes(name, sides):
            src, dst = red.at[block(dest), :], ret.at[block(sp), :]
            send(remote(src, dst, ret_s, ret_r.at[index[name]], dest, tp))

    def give_back(name):
        add_up(name)
        give(name)

    half = rows // 2

    def turn(h):
        part = pl.ds(pl.multiple_of(h * half, half), half)

        def step(j, carry):
            sl = pl.ds(pl.multiple_of(j * dcols, dcols), dcols)
            saved_t[sl, part] = jnp.transpose(saved[part, sl])
            return carry

        lax.fori_loop(0, width // dcols, step, 0)
        hidden_t[:, part] = jnp.transpose(hid[part, :])

    def down_tile(j, carry):
        sl = pl.ds(pl.multiple_of(j * dcols, dcols), dcols)
        gd_v[:, sl] = dot_nn(hidden_t[...], eg[:, sl]).astype(bf16)
        return carry

    tile = width // 8

    def weight_tile(j, carry):
        sl = pl.ds(pl.multiple_of(j * tile, tile), tile)
        x = saved_t[sl, :]
        gg_v[sl, :] = dot_nn(x, ggrad[...]).astype(bf16)
        gu_v[sl, :] = dot_nn(x, ugrad[...]).astype(bf16)
        return carry

    dispatch(("own", "mirror", "beyond", "near"))
    eg[block(sp), mine] = disp[block(sp), :]
    wd_load.wait()
    flip(wd, wd_t)
    wg_load.wait()
    flip(wg, wg_t)
    wu_load.wait()
    flip(wu, wu_t)
    lg_relay()
    select_across()
    dispatch_far(("own", "beyond", "near"))
    eg[block(sp), other] = disp_far[block(sp), :]
    eg_mine("mirror")
    saved_across("beyond")
    ein_load.wait()
    saved_relay("mirror")
    halo_copy = mixer()
    await_region(saved.at[:, cols(partner)], ein_s, ein_r.at[4])
    saved_arrive("mirror")
    forward("mirror")
    eg_mine("own")
    eg_other("own")
    saved_relay("own")
    saved_arrive("own")
    forward("own")
    eg_arrive("own")
    backward("own")
    eg_other("mirror")
    pass_on("own")
    eg_arrive("mirror")
    backward("mirror")
    pass_on("mirror")
    saved_across("near")
    saved_relay("beyond")
    eg_mine("beyond")
    saved_arrive("beyond")
    forward("beyond")
    turn(1 - lax.div(plane, 2))
    proj_near()
    eg_mine("near")
    eg_other("near")
    eg_other("beyond")
    give_back("mirror")
    eg_arrive("beyond")
    backward("beyond")
    pass_on("beyond")
    give_back("own")
    proj_mirror()
    saved_relay("near")
    saved_arrive("near")
    forward("near")
    eg_arrive("near")
    backward("near")
    pass_on("near")
    turn(lax.div(plane, 2))
    give_back("beyond")
    halo_copy.wait_recv()
    ext[tokens : tokens + 8, :] = jnp.where(sp < n_sp - 1, halo[...], 0.0)
    reach = taps_ref.shape[0] - 1
    tap_values = taps_ref[...].astype(f32)
    conv_grad = tap_values[0:1, :] * ext[reach : reach + tokens, :]
    for j in range(1, reach + 1):
        conv_grad = conv_grad + tap_values[j : j + 1, :] * ext[reach - j : reach - j + tokens, :]
    gci_ref[...] = (conv_grad * cg_ref[...].astype(f32)).astype(bf16)
    gcg_ref[...] = (conv_grad * ci_ref[...].astype(f32)).astype(bf16)
    lax.fori_loop(0, width // dcols, down_tile, 0)
    lax.fori_loop(0, 4, weight_tile, 0)
    give_back("near")
    lax.fori_loop(4, 8, weight_tile, 0)
    proj_total()
    def await_back(name):
        await_region(ret.at[rows_from(name), :], ret_s, ret_r.at[index[name]])
    await_back("mirror")
    await_back("beyond")
    await_back("near")
    await_back("own")
    sent(fg.at[:, 0 : 3 * dcols], lg_s)
    sent(saved.at[:, 0 : 3 * dcols], ein_s)
    sent(disp.at[0 : (n_sp - 1) * cap, :], disp_s)
    sent(disp_far.at[0 : (n_sp - 1 - 2 * len(EXCHANGED)) * cap, :], far_s)
    sent(eg.at[:, 0 : 2 * dcols], egs_s)
    for _ in EXCHANGED:
        sent(eg.at[0:pair, 0:dcols], swap_s)
    sent(px, d2d_s)
    sent(ysend, y_s)
    sent(red.at[0 : (n_sp - 1) * cap, :], ret_s)
    sent(proj_x, proj_s.at[0])
    sent(proj_n, proj_s.at[1])
    sent(proj_a, proj_s.at[2])
    halo_copy.wait_send()


def write_out(*refs):
    gate, up, down, sel, ret = refs[:5]
    ready, outs, total, sems = (gate, up, down) + refs[5:9], refs[9:17], refs[17], refs[18]
    copies = []
    for n, (src, dst) in enumerate(zip(ready, outs[:3] + outs[4:])):
        copies.append(pltpu.make_async_copy(src, dst, sems.at[n]))
    for copy in copies:
        copy.start()
    total[...] = dot_tn(sel[...], ret[...]).astype(bf16)
    last = pltpu.make_async_copy(total, outs[3], sems.at[len(copies)])
    last.start()
    for copy in copies + [last]:
        copy.wait()


def fused(n_sp, layer_grad, routes, route_weights, expert_in, w_gate, w_up, w_down,
          conv_in, c_gate, b_gate, conv_out, taps, w_out):
    tokens, dcols = layer_grad.shape
    rows = expert_in.shape[1]
    width, units = w_gate.shape[1:]
    chans = conv_in.shape[1]
    share = width // n_sp
    planes = n_sp // 2
    any_spec = pl.BlockSpec(memory_space=pl.ANY)
    vmem = pl.BlockSpec(memory_space=pltpu.VMEM)
    dma = pltpu.SemaphoreType.DMA
    shape = jax.ShapeDtypeStruct
    kinds = (
        ((width, units), bf16),
        ((width, units), bf16),
        ((units, width), bf16),
        ((rows, tokens), bf16),
        ((rows, dcols), bf16),
        ((chans, share), f32),
        ((tokens, chans), bf16),
        ((tokens, chans), bf16),
        ((tokens, chans), bf16),
    )
    results = pl.pallas_call(
        functools.partial(fused_kernel, n_sp),
        out_shape=tuple(pltpu.VMEM(dims, dtype) for dims, dtype in kinds),
        in_specs=[any_spec] * 13,
        out_specs=(vmem,) * len(kinds),
        scratch_shapes=[
            pltpu.VMEM((width, units), bf16),
            pltpu.VMEM((width, units), bf16),
            pltpu.VMEM((units, width), bf16),
            pltpu.VMEM((units, width), bf16),
            pltpu.VMEM((units, width), bf16),
            pltpu.VMEM((width, units), bf16),
            pltpu.VMEM((chans, width), bf16),
            pltpu.VMEM((tokens, width), bf16),
            pltpu.VMEM((rows, width), bf16),
            pltpu.VMEM((width, rows), bf16),
            pltpu.VMEM((rows, width), bf16),
            pltpu.VMEM((rows, dcols), bf16),
            pltpu.VMEM((rows, dcols), bf16),
            pltpu.VMEM((rows, 128), f32),
            pltpu.VMEM((2, planes, chans, share), f32),
            pltpu.VMEM((planes, chans, share), bf16),
            pltpu.VMEM((planes, chans, share), bf16),
            pltpu.VMEM((2, chans, share), bf16),
            pltpu.VMEM((2, chans, share), bf16),
            pltpu.VMEM((chans, share), bf16),
            pltpu.VMEM((chans, share), bf16),
            pltpu.VMEM((tokens + 8, chans), f32),
            pltpu.VMEM((8, chans), f32),
            pltpu.VMEM((rows, units), bf16),
            pltpu.VMEM((units, rows), bf16),
            pltpu.VMEM((rows, units), f32),
            pltpu.VMEM((rows, units), f32),
            pltpu.VMEM((rows, units), bf16),
            pltpu.VMEM((rows, units), bf16),
            pltpu.VMEM((rows, width), bf16),
            pltpu.VMEM((rows, 2 * dcols), bf16),
            pltpu.VMEM((rows, dcols), bf16),
            pltpu.VMEM((rows, dcols), bf16),
            pltpu.VMEM((rows, dcols), bf16),
            pltpu.VMEM(routes.shape[::-1], jnp.int32),
            pltpu.VMEM(routes.shape[::-1], f32),
            pltpu.VMEM((tokens, chans), bf16),
            pltpu.VMEM((tokens, chans), bf16),
            pltpu.VMEM((tokens, chans), bf16),
            pltpu.VMEM((tokens, chans), bf16),
            pltpu.VMEM(taps.shape, bf16),
            dma((13,)),
            dma,
            dma((3,)),
            dma,
            dma((9,)),
            dma,
            dma((4,)),
            dma,
            dma((4,)),
            dma,
            dma((8,)),
            dma,
            dma((2,)),
            dma((3,)),
            dma((3,)),
            dma,
            dma,
            dma,
            dma((4,)),
            dma,
            dma((4,)),
            dma,
            dma((4,)),
        ],
        compiler_params=pltpu.CompilerParams(
            collective_id=0, has_side_effects=True, vmem_limit_bytes=52 * 1024 * 1024
        ),
    )(
        layer_grad,
        routes.T,
        route_weights.T,
        expert_in[0],
        w_gate[0],
        w_up[0],
        w_down[0],
        conv_in,
        c_gate,
        b_gate,
        conv_out,
        taps,
        w_out,
    )
    results = pl.pallas_call(
        write_out,
        out_shape=tuple(
            shape(dims, dtype)
            for dims, dtype in kinds[:3] + (((tokens, dcols), bf16),) + kinds[5:]
        ),
        in_specs=[vmem] * len(kinds),
        out_specs=(any_spec,) * (len(kinds) - 1),
        scratch_shapes=[pltpu.VMEM((tokens, dcols), bf16), dma((len(kinds) - 1,))],
        compiler_params=pltpu.CompilerParams(vmem_limit_bytes=2 * 1024 * 1024),
    )(*results)
    gate, up, down = results[:3]
    return (gate[None], up[None], down[None]) + tuple(results[3:])


def dispatching(n_sp, n_tp, layer_grad, routes, route_weights, expert_in, *others):
    tokens, dcols = layer_grad.shape
    cap = expert_in.shape[1] // n_sp
    chans = others[3].shape[1]
    fits = (
        n_tp == 4
        and n_sp == 8
        and cap % 16 == 0
        and tokens % 128 == 0
        and dcols % 128 == 0
        and chans % 128 == 0
        and (dcols * n_tp) % (n_sp * 128) == 0
        and others[-2].shape[0] <= 9
    )
    if fits:
        return fused(n_sp, layer_grad, routes, route_weights, expert_in, *others)
    return per_device(layer_grad, routes, route_weights, expert_in, *others)


def solution(mesh):
    in_specs = (
        P("sp", "tp"),
        P("sp", None),
        P("sp", None),
        P("sp", None, "tp"),
        P("sp", None, "tp"),
        P("sp", None, "tp"),
        P("sp", "tp", None),
        P("sp", "tp"),
        P("sp", "tp"),
        P("sp", "tp"),
        P("sp", "tp"),
        P(None, "tp"),
        P("tp", None),
    )
    out_specs = (
        P("sp", None, "tp"),
        P("sp", None, "tp"),
        P("sp", "tp", None),
        P("sp", "tp"),
        P("tp", "sp"),
        P("sp", "tp"),
        P("sp", "tp"),
        P("sp", "tp"),
    )
    return jax.shard_map(
        functools.partial(dispatching, mesh.shape["sp"], mesh.shape["tp"]), mesh=mesh, in_specs=in_specs, out_specs=out_specs, check_vma=False
    )
```

```python
import functools

import jax
import jax.numpy as jnp
from jax import lax
from jax.experimental import pallas as pl
from jax.experimental.pallas import tpu as pltpu
from jax.sharding import PartitionSpec as P

clamp_limit = 7.0
swish_alpha = 1.702


def passed_along(value, axis, steps):
    count = lax.axis_size(axis)
    leading, last = (max(0, -steps), min(count, count - steps))
    return lax.ppermute(value, axis, [(source, source + steps) for source in range(leading, last)])


def per_device(
    layer_grad,
    routes,
    route_weights,
    expert_in,
    w_gate,
    w_up,
    w_down,
    conv_in,
    c_gate,
    b_gate,
    conv_out,
    taps,
    w_out,
):
    sp_devices = lax.axis_size("sp")
    tok_rows = layer_grad.shape[0]
    top_count = routes.shape[1]
    capacity = expert_in.shape[1] // sp_devices
    full_grad = lax.all_gather(layer_grad, "tp", axis=1, tiled=True)
    flat_routes = routes.reshape(-1)
    onehot = (flat_routes[:, None] == jnp.arange(sp_devices, dtype=jnp.int32)[None, :]).astype(
        jnp.int32
    )
    slot_rank = jnp.sum((jnp.cumsum(onehot, axis=0) - 1) * onehot, axis=1)
    slot_index = flat_routes * capacity + slot_rank
    weights = route_weights[:, :, None]
    scaled = (weights * layer_grad[:, None, :].astype(jnp.float32)).astype(jnp.bfloat16)
    scaled = scaled.reshape(tok_rows * top_count, -1)
    buffer = (
        jnp.zeros((sp_devices * capacity, scaled.shape[1]), jnp.bfloat16).at[slot_index].set(scaled)
    )
    arrived = lax.all_to_all(
        buffer.reshape(sp_devices, capacity, -1), "sp", split_axis=0, concat_axis=0, tiled=True
    )
    expert_grad, saved_rows = (
        lax.all_gather(arrived.reshape(sp_devices * capacity, -1), "tp", axis=1, tiled=True),
        lax.all_gather(expert_in[0], "tp", axis=1, tiled=True),
    )
    gate_weight = w_gate[0]
    up_weight = w_up[0]
    down_weight = w_down[0]
    gate_pre = jnp.dot(saved_rows, gate_weight, preferred_element_type=jnp.float32)
    up_pre = jnp.dot(saved_rows, up_weight, preferred_element_type=jnp.float32)
    gate_cut = jnp.minimum(gate_pre, clamp_limit)
    up_cut = jnp.clip(up_pre, -clamp_limit, clamp_limit)
    sigmoid_gate = jax.nn.sigmoid(swish_alpha * gate_cut)
    hidden = ((up_cut + 1.0) * gate_cut * sigmoid_gate).astype(jnp.bfloat16)
    act_grad = jnp.einsum("rd,fd->rf", expert_grad, down_weight, preferred_element_type=jnp.float32)
    grad_down = jnp.einsum(
        "rf,rd->fd", hidden, expert_grad, preferred_element_type=jnp.float32
    ).astype(jnp.bfloat16)
    slope = sigmoid_gate + swish_alpha * gate_cut * sigmoid_gate * (1.0 - sigmoid_gate)
    gate_grad = jnp.where(gate_pre < clamp_limit, act_grad * (up_cut + 1.0) * slope, 0.0).astype(
        jnp.bfloat16
    )
    up_grad = jnp.where(
        jnp.abs(up_pre) < clamp_limit, act_grad * gate_cut * sigmoid_gate, 0.0
    ).astype(jnp.bfloat16)
    grad_gate = jnp.einsum(
        "rd,rf->df", saved_rows, gate_grad, preferred_element_type=jnp.float32
    ).astype(jnp.bfloat16)
    grad_up = jnp.einsum(
        "rd,rf->df", saved_rows, up_grad, preferred_element_type=jnp.float32
    ).astype(jnp.bfloat16)
    partial_value = jnp.einsum(
        "rf,df->rd", gate_grad, gate_weight, preferred_element_type=jnp.float32
    )
    partial_value = partial_value + jnp.einsum(
        "rf,df->rd", up_grad, up_weight, preferred_element_type=jnp.float32
    )
    rounded_terms = partial_value.astype(jnp.bfloat16)
    reduced = (
        lax.psum_scatter(rounded_terms, "tp", scatter_dimension=1, tiled=True)
        .astype(jnp.float32)
        .astype(jnp.bfloat16)
    )
    returned = lax.all_to_all(
        reduced.reshape(sp_devices, capacity, -1), "sp", split_axis=0, concat_axis=0, tiled=True
    )
    returned = returned.reshape(sp_devices * capacity, -1)
    picked = returned[slot_index]
    picked = picked.reshape(tok_rows, top_count, -1)
    grad_routed = jnp.sum(picked.astype(jnp.float32), axis=1).astype(jnp.bfloat16)
    mixer_grad = jnp.einsum("td,cd->tc", full_grad, w_out, preferred_element_type=jnp.float32)
    mixed = (b_gate.astype(jnp.float32) * conv_out.astype(jnp.float32)).astype(jnp.bfloat16)
    projected = lax.psum_scatter(
        jnp.einsum("td,tc->dc", full_grad, mixed, preferred_element_type=jnp.float32),
        "sp",
        scatter_dimension=0,
        tiled=True,
    )
    grad_out_proj = projected.T
    out_grad = mixer_grad * b_gate.astype(jnp.float32)
    tap_reach = taps.shape[0] - 1
    following = passed_along(out_grad[:tap_reach], "sp", -1)
    extended = jnp.concatenate([out_grad, following], axis=0)
    tap_values = taps.astype(jnp.float32)
    conv_grad = jnp.zeros_like(out_grad)
    for tap_index in range(tap_reach + 1):
        offset = tap_reach - tap_index
        conv_grad = conv_grad + tap_values[tap_index] * extended[offset : offset + tok_rows]
    grad_conv_in = (conv_grad * c_gate.astype(jnp.float32)).astype(jnp.bfloat16)
    grad_c_gate = (conv_grad * conv_in.astype(jnp.float32)).astype(jnp.bfloat16)
    grad_b_gate = (mixer_grad * conv_out.astype(jnp.float32)).astype(jnp.bfloat16)
    return (
        grad_gate[None],
        grad_up[None],
        grad_down[None],
        grad_routed,
        grad_out_proj,
        grad_conv_in,
        grad_c_gate,
        grad_b_gate,
    )


MESH = pl.DeviceIdType.MESH
bf16 = jnp.bfloat16
f32 = jnp.float32


def dot_nn(a, b):
    return jnp.dot(a, b, preferred_element_type=f32)


def dot_nt(a, b):
    return lax.dot_general(a, b, (((1,), (1,)), ((), ())), preferred_element_type=f32)


def dot_tn(a, b):
    return lax.dot_general(a, b, (((0,), (0,)), ((), ())), preferred_element_type=f32)


EXCHANGED = ("mirror",)
EARLY = "own"
FIRST_SAVED = ("own", "mirror", "beyond")


def fused_kernel(
    n_sp,
    lg_hbm,
    rt_hbm,
    wt_hbm,
    ein_hbm,
    wg_hbm,
    wu_hbm,
    wd_hbm,
    ci_hbm,
    cg_hbm,
    bg_hbm,
    co_hbm,
    taps_hbm,
    wo_hbm,
    gg_v,
    gu_v,
    gd_v,
    sel,
    ret,
    gop_ref,
    gci_ref,
    gcg_ref,
    gbg_ref,
    wg,
    wu,
    wd,
    wg_t,
    wu_t,
    wd_t,
    wo,
    fg,
    saved,
    saved_t,
    eg,
    disp,
    disp_far,
    row_scale,
    proj,
    proj_x,
    proj_xr,
    proj_n,
    proj_nr,
    proj_a,
    proj_ar,
    ext,
    halo,
    hid,
    hidden_t,
    fac_g,
    fac_u,
    ggrad,
    ugrad,
    terms,
    px,
    ysend,
    yrecv,
    red,
    rt_ref,
    wt_ref,
    ci_ref,
    cg_ref,
    bg_ref,
    co_ref,
    taps_ref,
    load_s,
    lg_s,
    lg_r,
    ein_s,
    ein_r,
    disp_s,
    disp_r,
    far_s,
    far_r,
    egs_s,
    egs_r,
    swap_s,
    swap_r,
    proj_s,
    proj_r,
    halo_s,
    halo_r,
    d2d_s,
    d2d_r,
    y_s,
    y_r,
    ret_s,
    ret_r,
):
    sp = lax.axis_index("sp")
    tp = lax.axis_index("tp")
    core, chip = lax.rem(tp, 2), lax.div(tp, 2)
    partner = chip * 2 + (1 - core)
    across = (1 - chip) * 2 + core
    plane, side = lax.div(sp, 2), lax.rem(sp, 2)
    planes = n_sp // 2
    sibling = plane * 2 + (1 - side)
    near = plane + 1 - 2 * lax.rem(plane, 2)
    mirror = lax.rem(plane + 2, planes)
    beyond = lax.rem(near + 2, planes)
    rows, dcols = ein_hbm.shape
    cap = rows // n_sp
    pair = 2 * cap
    width = fg.shape[1]
    tokens = fg.shape[0]
    top = rt_hbm.shape[0]
    quads = {"own": plane, "near": near, "mirror": mirror, "beyond": beyond}
    index = {"own": 0, "near": 1, "mirror": 2, "beyond": 3}

    def cols(j):
        return pl.ds(pl.multiple_of(j * dcols, dcols), dcols)

    def block(b):
        return pl.ds(pl.multiple_of(b * cap, cap), cap)

    def pair_rows(q):
        return pl.ds(pl.multiple_of(q * pair, pair), pair)

    mine, other = cols(tp), cols(across)
    corner = cols((1 - chip) * 2 + (1 - core))

    def load(src, dst, n):
        copy = pltpu.make_async_copy(src, dst, load_s.at[n])
        copy.start()
        return copy

    def remote(src, dst, send, recv, to_sp, to_tp):
        return pltpu.make_async_remote_copy(
            src_ref=src,
            dst_ref=dst,
            send_sem=send,
            recv_sem=recv,
            device_id=(to_sp, to_tp),
            device_id_type=MESH,
        )

    barrier = pltpu.get_barrier_semaphore()
    pl.semaphore_signal(barrier, inc=1, device_id=(sp, partner), device_id_type=MESH)
    pl.semaphore_signal(barrier, inc=1, device_id=(sp, across), device_id_type=MESH)
    for i in range(1, n_sp):
        pl.semaphore_signal(
            barrier, inc=1, device_id=(lax.rem(sp + i, n_sp), tp), device_id_type=MESH
        )
    lg_load = load(lg_hbm, fg.at[:, mine], 0)
    ein_load = load(ein_hbm, saved.at[:, mine], 1)
    route_load = load(rt_hbm, rt_ref, 6)
    weight_load = load(wt_hbm, wt_ref, 7)
    mixer_loads = [
        load(bg_hbm, bg_ref, 8),
        load(co_hbm, co_ref, 9),
        load(ci_hbm, ci_ref, 10),
        load(cg_hbm, cg_ref, 11),
        load(taps_hbm, taps_ref, 12),
    ]
    wo_load = load(wo_hbm, wo, 2)
    wg_load = load(wg_hbm, wg, 3)
    wu_load = load(wu_hbm, wu, 4)
    wd_load = load(wd_hbm, wd, 5)
    pl.semaphore_wait(barrier, n_sp + 1)

    def send(copy):
        copy.start()
        return copy

    def sent(region, sem):
        remote(region, region, sem, sem, sp, partner).wait_send()

    def await_region(region, s_sem, r_sem):
        remote(region, region, s_sem, r_sem, sp, partner).wait_recv()

    def saved_across(name, sides=(0, 1)):
        i = index[name]
        for x in sides:
            sl = block(quads[name] * 2 + x)
            dst = saved.at[sl, mine]
            send(remote(ein_hbm.at[sl, :], dst, ein_s, ein_r.at[i], sp, across))

    def saved_relay(name):
        region, i = saved.at[pair_rows(quads[name]), other], index[name]
        await_region(region, ein_s, ein_r.at[i])
        send(remote(region, region, ein_s, ein_r.at[5 + i], sp, partner))

    def saved_arrive(name):
        region = saved.at[pair_rows(quads[name]), corner]
        await_region(region, ein_s, ein_r.at[5 + index[name]])

    def homes(name, sides=(0, 1)):
        return [sibling] if name == "own" else [quads[name] * 2 + x for x in sides]

    def rows_from(name):
        return block(sibling) if name == "own" else pair_rows(quads[name])

    send(remote(lg_hbm, fg.at[:, mine], lg_s, lg_r.at[0], sp, across))
    saved_across("mirror")
    saved_across(EARLY)
    send(remote(lg_hbm, fg.at[:, mine], lg_s, lg_r.at[1], sp, partner))
    send(remote(ein_hbm, saved.at[:, mine], ein_s, ein_r.at[4], sp, partner))

    route_load.wait()
    weight_load.wait()
    expert_ids = lax.broadcasted_iota(jnp.int32, (n_sp, tokens), 0)
    named = jnp.zeros((n_sp, tokens), f32)
    weight = jnp.zeros((n_sp, tokens), f32)
    for k in range(top):
        hit = rt_ref[k : k + 1, :] == expert_ids
        named = jnp.where(hit, 1.0, named)
        weight = jnp.where(hit, wt_ref[k : k + 1, :], weight)
    earlier = (
        lax.broadcasted_iota(jnp.int32, (tokens, tokens), 0)
        < lax.broadcasted_iota(jnp.int32, (tokens, tokens), 1)
    )
    rank = dot_nn(named.astype(bf16), jnp.where(earlier, 1.0, 0.0).astype(bf16))
    rank = jnp.where(named > 0.0, rank, -1.0)
    slots = lax.broadcasted_iota(jnp.int32, (cap, tokens), 0).astype(f32)
    lg_load.wait()
    own_grad = fg[:, mine]
    for e in range(n_sp):
        chosen = slots == rank[e : e + 1, :]
        picks = jnp.where(chosen, 1.0, 0.0)
        row_weight = jnp.sum(jnp.where(chosen, weight[e : e + 1, :], 0.0), axis=1, keepdims=True)
        here = slice(e * cap, (e + 1) * cap)
        sel[here, :] = picks.astype(bf16)
        row_scale[here, :] = jnp.broadcast_to(row_weight, (cap, row_scale.shape[1]))
        disp[here, :] = (dot_nn(picks.astype(bf16), own_grad) * row_weight).astype(bf16)

    def dispatch(names):
        for name in names:
            for dest in homes(name):
                src, dst = disp.at[block(dest), :], eg.at[block(sp), mine]
                send(remote(src, dst, disp_s, disp_r.at[index[name]], dest, tp))

    def dispatch_far(names):
        for name in names:
            for dest in homes(name):
                src, dst = disp_far.at[block(dest), :], eg.at[block(sp), other]
                send(remote(src, dst, far_s, far_r.at[index[name]], dest, tp))

    def lg_relay():
        await_region(fg.at[:, other], lg_s, lg_r.at[0])
        send(remote(fg.at[:, other], fg.at[:, other], lg_s, lg_r.at[2], sp, partner))

    def select_across():
        far_grad = fg[:, other]
        for e in range(n_sp):
            here = slice(e * cap, (e + 1) * cap)
            disp_far[here, :] = (dot_nn(sel[here, :], far_grad) * row_scale[here, 0:1]).astype(bf16)

    def flip(src, dst):
        step = 512

        def part(j, carry):
            sl = pl.ds(pl.multiple_of(j * step, step), step)
            if src.shape[0] > src.shape[1]:
                dst[:, sl] = jnp.transpose(src[sl, :])
            else:
                dst[sl, :] = jnp.transpose(src[:, sl])
            return carry

        lax.fori_loop(0, width // step, part, 0)

    share = width // n_sp

    def mixer():
        wo_load.wait()
        for one in mixer_loads:
            one.wait()
        await_region(fg.at[:, cols(partner)], lg_s, lg_r.at[1])
        await_region(fg.at[:, corner], lg_s, lg_r.at[2])
        b_gate = bg_ref[...].astype(f32)
        conv_out = co_ref[...].astype(f32)
        mixer_grad = dot_nt(fg[...], wo[...])
        ext[0:tokens, :] = mixer_grad * b_gate
        gbg_ref[...] = (mixer_grad * conv_out).astype(bf16)
        before = lax.rem(sp + n_sp - 1, n_sp)
        halo_copy = send(remote(ext.at[0:8, :], halo, halo_s, halo_r, before, tp))
        mixed = (b_gate * conv_out).astype(bf16)
        for d in range(n_sp):
            proj[d % 2, d // 2] = dot_tn(mixed, fg[:, d * share : (d + 1) * share])
        proj_x[...] = proj[1 - side].astype(bf16)
        send(remote(proj_x, proj_xr, proj_s.at[0], proj_r.at[0], sibling, tp))
        return halo_copy

    def proj_near():
        await_region(proj_xr, proj_s.at[0], proj_r.at[0])
        for q in range(planes):
            proj[0, q] = proj[side, q] + proj_xr[q].astype(f32)
        proj_n[0] = proj[0, near].astype(bf16)
        proj_n[1] = proj[0, beyond].astype(bf16)
        send(remote(proj_n, proj_nr, proj_s.at[1], proj_r.at[1], near * 2 + side, tp))

    def proj_mirror():
        await_region(proj_nr, proj_s.at[1], proj_r.at[1])
        proj_a[...] = (proj[0, mirror] + proj_nr[1].astype(f32)).astype(bf16)
        send(remote(proj_a, proj_ar, proj_s.at[2], proj_r.at[2], mirror * 2 + side, tp))

    def proj_total():
        await_region(proj_ar, proj_s.at[2], proj_r.at[2])
        gop_ref[...] = proj[0, plane] + proj_nr[0].astype(f32) + proj_ar[...].astype(f32)

    def eg_mine(name):
        i, region = index[name], eg.at[pair_rows(quads[name]), mine]
        await_region(eg.at[rows_from(name), mine], disp_s, disp_r.at[i])
        if name in EXCHANGED:
            send(remote(region, region, swap_s, swap_r.at[EXCHANGED.index(name)], sp, across))
        send(remote(region, region, egs_s, egs_r.at[i], sp, partner))

    def eg_other(name):
        i, region = index[name], eg.at[pair_rows(quads[name]), other]
        if name in EXCHANGED:
            await_region(region, swap_s, swap_r.at[EXCHANGED.index(name)])
        else:
            await_region(eg.at[rows_from(name), other], far_s, far_r.at[i])
        send(remote(region, region, egs_s, egs_r.at[4 + i], sp, partner))

    def eg_arrive(name):
        sl, i = pair_rows(quads[name]), index[name]
        await_region(eg.at[sl, cols(partner)], egs_s, egs_r.at[i])
        await_region(eg.at[sl, corner], egs_s, egs_r.at[4 + i])

    def forward(name):
        sl = pair_rows(quads[name])
        x = saved[sl, :]
        gate_pre = dot_nn(x, wg[...])
        up_pre = dot_nn(x, wu[...])
        gate_cut = jnp.minimum(gate_pre, clamp_limit)
        up_cut = jnp.clip(up_pre, -clamp_limit, clamp_limit)
        sig = jax.nn.sigmoid(swish_alpha * gate_cut)
        base = gate_cut * sig
        slope = sig + swish_alpha * base * (1.0 - sig)
        hid[sl, :] = ((up_cut + 1.0) * base).astype(bf16)
        fac_g[sl, :] = jnp.where(gate_pre < clamp_limit, (up_cut + 1.0) * slope, 0.0)
        fac_u[sl, :] = jnp.where(jnp.abs(up_pre) < clamp_limit, base, 0.0)

    def backward(name):
        sl, i = pair_rows(quads[name]), index[name]
        act_grad = dot_nn(eg[sl, :], wd_t[...])
        g = (act_grad * fac_g[sl, :]).astype(bf16)
        u = (act_grad * fac_u[sl, :]).astype(bf16)
        ggrad[sl, :] = g
        ugrad[sl, :] = u

        def term(m):
            j = cols(m)
            terms[sl, j] = (dot_nn(g, wg_t[:, j]) + dot_nn(u, wu_t[:, j])).astype(bf16)

        for y in range(2):
            there = y * 2 + (1 - core)
            term(there)
            send(
                remote(
                    terms.at[sl, cols(there)],
                    px.at[sl, y * dcols : (y + 1) * dcols],
                    d2d_s,
                    d2d_r.at[i],
                    sp,
                    partner,
                )
            )
        for y in range(2):
            term(y * 2 + core)

    def pass_on(name, sides=(0, 1)):
        sl, i = pair_rows(quads[name]), index[name]
        if 0 in sides:
            await_region(px.at[sl, :], d2d_s, d2d_r.at[i])
        if len(sides) == 1:
            sl = block(quads[name] * 2 + sides[0])
        far = terms[sl, other].astype(f32) + px[sl, cols(1 - chip)].astype(f32)
        ysend[sl, :] = far.astype(bf16)
        send(remote(ysend.at[sl, :], yrecv.at[sl, :], y_s, y_r.at[i], sp, across))

    def add_up(name):
        sl, i = pair_rows(quads[name]), index[name]
        await_region(yrecv.at[sl, :], y_s, y_r.at[i])
        near_sum = terms[sl, mine].astype(f32) + px[sl, cols(chip)].astype(f32)
        red[sl, :] = (near_sum + yrecv[sl, :].astype(f32)).astype(bf16)
        if name == "own":
            ret[block(sp), :] = red[block(sp), :]

    def give(name, sides=(0, 1)):
        for dest in homes(name, sides):
            src, dst = red.at[block(dest), :], ret.at[block(sp), :]
            send(remote(src, dst, ret_s, ret_r.at[index[name]], dest, tp))

    def give_back(name):
        add_up(name)
        give(name)

    half = rows // 2

    def turn(h):
        part = pl.ds(pl.multiple_of(h * half, half), half)

        def step(j, carry):
            sl = pl.ds(pl.multiple_of(j * dcols, dcols), dcols)
            saved_t[sl, part] = jnp.transpose(saved[part, sl])
            return carry

        lax.fori_loop(0, width // dcols, step, 0)
        hidden_t[:, part] = jnp.transpose(hid[part, :])

    def down_tile(j, carry):
        sl = pl.ds(pl.multiple_of(j * dcols, dcols), dcols)
        gd_v[:, sl] = dot_nn(hidden_t[...], eg[:, sl]).astype(bf16)
        return carry

    tile = width // 8

    def weight_tile(j, carry):
        sl = pl.ds(pl.multiple_of(j * tile, tile), tile)
        x = saved_t[sl, :]
        gg_v[sl, :] = dot_nn(x, ggrad[...]).astype(bf16)
        gu_v[sl, :] = dot_nn(x, ugrad[...]).astype(bf16)
        return carry

    dispatch(("own", "mirror", "near", "beyond"))
    eg[block(sp), mine] = disp[block(sp), :]
    wd_load.wait()
    flip(wd, wd_t)
    wg_load.wait()
    flip(wg, wg_t)
    wu_load.wait()
    flip(wu, wu_t)
    lg_relay()
    select_across()
    dispatch_far(("own", "near", "beyond"))
    eg[block(sp), other] = disp_far[block(sp), :]
    ein_load.wait()
    saved_relay("mirror")
    halo_copy = mixer()
    eg_mine("mirror")
    saved_across("near")
    saved_across("beyond")
    await_region(saved.at[:, cols(partner)], ein_s, ein_r.at[4])
    saved_arrive("mirror")
    forward("mirror")
    eg_mine("own")
    eg_other("own")
    saved_relay("own")
    saved_arrive("own")
    forward("own")
    eg_arrive("own")
    backward("own")
    eg_other("mirror")
    eg_mine("near")
    eg_other("near")
    eg_arrive("mirror")
    backward("mirror")
    saved_relay("near")
    pass_on("mirror")
    proj_near()
    saved_arrive("near")
    forward("near")
    eg_arrive("near")
    backward("near")
    pass_on("near")
    proj_mirror()
    saved_relay("beyond")
    eg_mine("beyond")
    eg_other("beyond")
    turn(lax.div(plane, 2))
    saved_arrive("beyond")
    forward("beyond")
    give_back("mirror")
    eg_arrive("beyond")
    backward("beyond")
    pass_on("beyond")
    pass_on("own")
    turn(1 - lax.div(plane, 2))
    halo_copy.wait_recv()
    ext[tokens : tokens + 8, :] = jnp.where(sp < n_sp - 1, halo[...], 0.0)
    reach = taps_ref.shape[0] - 1
    tap_values = taps_ref[...].astype(f32)
    conv_grad = tap_values[0:1, :] * ext[reach : reach + tokens, :]
    for j in range(1, reach + 1):
        conv_grad = conv_grad + tap_values[j : j + 1, :] * ext[reach - j : reach - j + tokens, :]
    gci_ref[...] = (conv_grad * cg_ref[...].astype(f32)).astype(bf16)
    gcg_ref[...] = (conv_grad * ci_ref[...].astype(f32)).astype(bf16)
    lax.fori_loop(0, width // dcols, down_tile, 0)
    give_back("near")
    lax.fori_loop(0, 4, weight_tile, 0)
    give_back("beyond")
    lax.fori_loop(4, 8, weight_tile, 0)
    give_back("own")
    proj_total()
    def await_back(name):
        await_region(ret.at[rows_from(name), :], ret_s, ret_r.at[index[name]])
    await_back("mirror")
    await_back("near")
    await_back("own")
    await_back("beyond")
    sent(fg.at[:, 0 : 3 * dcols], lg_s)
    sent(saved.at[:, 0 : 3 * dcols], ein_s)
    sent(disp.at[0 : (n_sp - 1) * cap, :], disp_s)
    sent(disp_far.at[0 : (n_sp - 1 - 2 * len(EXCHANGED)) * cap, :], far_s)
    sent(eg.at[:, 0 : 2 * dcols], egs_s)
    for _ in EXCHANGED:
        sent(eg.at[0:pair, 0:dcols], swap_s)
    sent(px, d2d_s)
    sent(ysend, y_s)
    sent(red.at[0 : (n_sp - 1) * cap, :], ret_s)
    sent(proj_x, proj_s.at[0])
    sent(proj_n, proj_s.at[1])
    sent(proj_a, proj_s.at[2])
    halo_copy.wait_send()


def write_out(*refs):
    gate, up, down, sel, ret = refs[:5]
    ready, outs, total, sems = (gate, up, down) + refs[5:9], refs[9:17], refs[17], refs[18]
    copies = []
    for n, (src, dst) in enumerate(zip(ready, outs[:3] + outs[4:])):
        copies.append(pltpu.make_async_copy(src, dst, sems.at[n]))
    for copy in copies:
        copy.start()
    total[...] = dot_tn(sel[...], ret[...]).astype(bf16)
    last = pltpu.make_async_copy(total, outs[3], sems.at[len(copies)])
    last.start()
    for copy in copies + [last]:
        copy.wait()


def fused(n_sp, layer_grad, routes, route_weights, expert_in, w_gate, w_up, w_down,
          conv_in, c_gate, b_gate, conv_out, taps, w_out):
    tokens, dcols = layer_grad.shape
    rows = expert_in.shape[1]
    width, units = w_gate.shape[1:]
    chans = conv_in.shape[1]
    share = width // n_sp
    planes = n_sp // 2
    any_spec = pl.BlockSpec(memory_space=pl.ANY)
    vmem = pl.BlockSpec(memory_space=pltpu.VMEM)
    dma = pltpu.SemaphoreType.DMA
    shape = jax.ShapeDtypeStruct
    kinds = (
        ((width, units), bf16),
        ((width, units), bf16),
        ((units, width), bf16),
        ((rows, tokens), bf16),
        ((rows, dcols), bf16),
        ((chans, share), f32),
        ((tokens, chans), bf16),
        ((tokens, chans), bf16),
        ((tokens, chans), bf16),
    )
    results = pl.pallas_call(
        functools.partial(fused_kernel, n_sp),
        out_shape=tuple(pltpu.VMEM(dims, dtype) for dims, dtype in kinds),
        in_specs=[any_spec] * 13,
        out_specs=(vmem,) * len(kinds),
        scratch_shapes=[
            pltpu.VMEM((width, units), bf16),
            pltpu.VMEM((width, units), bf16),
            pltpu.VMEM((units, width), bf16),
            pltpu.VMEM((units, width), bf16),
            pltpu.VMEM((units, width), bf16),
            pltpu.VMEM((width, units), bf16),
            pltpu.VMEM((chans, width), bf16),
            pltpu.VMEM((tokens, width), bf16),
            pltpu.VMEM((rows, width), bf16),
            pltpu.VMEM((width, rows), bf16),
            pltpu.VMEM((rows, width), bf16),
            pltpu.VMEM((rows, dcols), bf16),
            pltpu.VMEM((rows, dcols), bf16),
            pltpu.VMEM((rows, 128), f32),
            pltpu.VMEM((2, planes, chans, share), f32),
            pltpu.VMEM((planes, chans, share), bf16),
            pltpu.VMEM((planes, chans, share), bf16),
            pltpu.VMEM((2, chans, share), bf16),
            pltpu.VMEM((2, chans, share), bf16),
            pltpu.VMEM((chans, share), bf16),
            pltpu.VMEM((chans, share), bf16),
            pltpu.VMEM((tokens + 8, chans), f32),
            pltpu.VMEM((8, chans), f32),
            pltpu.VMEM((rows, units), bf16),
            pltpu.VMEM((units, rows), bf16),
            pltpu.VMEM((rows, units), f32),
            pltpu.VMEM((rows, units), f32),
            pltpu.VMEM((rows, units), bf16),
            pltpu.VMEM((rows, units), bf16),
            pltpu.VMEM((rows, width), bf16),
            pltpu.VMEM((rows, 2 * dcols), bf16),
            pltpu.VMEM((rows, dcols), bf16),
            pltpu.VMEM((rows, dcols), bf16),
            pltpu.VMEM((rows, dcols), bf16),
            pltpu.VMEM(routes.shape[::-1], jnp.int32),
            pltpu.VMEM(routes.shape[::-1], f32),
            pltpu.VMEM((tokens, chans), bf16),
            pltpu.VMEM((tokens, chans), bf16),
            pltpu.VMEM((tokens, chans), bf16),
            pltpu.VMEM((tokens, chans), bf16),
            pltpu.VMEM(taps.shape, bf16),
            dma((13,)),
            dma,
            dma((3,)),
            dma,
            dma((9,)),
            dma,
            dma((4,)),
            dma,
            dma((4,)),
            dma,
            dma((8,)),
            dma,
            dma((2,)),
            dma((3,)),
            dma((3,)),
            dma,
            dma,
            dma,
            dma((4,)),
            dma,
            dma((4,)),
            dma,
            dma((4,)),
        ],
        compiler_params=pltpu.CompilerParams(
            collective_id=0, has_side_effects=True, vmem_limit_bytes=52 * 1024 * 1024
        ),
    )(
        layer_grad,
        routes.T,
        route_weights.T,
        expert_in[0],
        w_gate[0],
        w_up[0],
        w_down[0],
        conv_in,
        c_gate,
        b_gate,
        conv_out,
        taps,
        w_out,
    )
    results = pl.pallas_call(
        write_out,
        out_shape=tuple(
            shape(dims, dtype)
            for dims, dtype in kinds[:3] + (((tokens, dcols), bf16),) + kinds[5:]
        ),
        in_specs=[vmem] * len(kinds),
        out_specs=(any_spec,) * (len(kinds) - 1),
        scratch_shapes=[pltpu.VMEM((tokens, dcols), bf16), dma((len(kinds) - 1,))],
        compiler_params=pltpu.CompilerParams(vmem_limit_bytes=2 * 1024 * 1024),
    )(*results)
    gate, up, down = results[:3]
    return (gate[None], up[None], down[None]) + tuple(results[3:])


def dispatching(n_sp, n_tp, layer_grad, routes, route_weights, expert_in, *others):
    tokens, dcols = layer_grad.shape
    cap = expert_in.shape[1] // n_sp
    chans = others[3].shape[1]
    fits = (
        n_tp == 4
        and n_sp == 8
        and cap % 16 == 0
        and tokens % 128 == 0
        and dcols % 128 == 0
        and chans % 128 == 0
        and (dcols * n_tp) % (n_sp * 128) == 0
        and others[-2].shape[0] <= 9
    )
    if fits:
        return fused(n_sp, layer_grad, routes, route_weights, expert_in, *others)
    return per_device(layer_grad, routes, route_weights, expert_in, *others)


def solution(mesh):
    in_specs = (
        P("sp", "tp"),
        P("sp", None),
        P("sp", None),
        P("sp", None, "tp"),
        P("sp", None, "tp"),
        P("sp", None, "tp"),
        P("sp", "tp", None),
        P("sp", "tp"),
        P("sp", "tp"),
        P("sp", "tp"),
        P("sp", "tp"),
        P(None, "tp"),
        P("tp", None),
    )
    out_specs = (
        P("sp", None, "tp"),
        P("sp", None, "tp"),
        P("sp", "tp", None),
        P("sp", "tp"),
        P("tp", "sp"),
        P("sp", "tp"),
        P("sp", "tp"),
        P("sp", "tp"),
    )
    return jax.shard_map(
        functools.partial(dispatching, mesh.shape["sp"], mesh.shape["tp"]), mesh=mesh, in_specs=in_specs, out_specs=out_specs, check_vma=False
    )
```

```python
import functools

import jax
import jax.numpy as jnp
from jax import lax
from jax.experimental import pallas as pl
from jax.experimental.pallas import tpu as pltpu
from jax.sharding import PartitionSpec as P

clamp_limit = 7.0
swish_alpha = 1.702


def passed_along(value, axis, steps):
    count = lax.axis_size(axis)
    leading, last = (max(0, -steps), min(count, count - steps))
    return lax.ppermute(value, axis, [(source, source + steps) for source in range(leading, last)])


def per_device(
    layer_grad,
    routes,
    route_weights,
    expert_in,
    w_gate,
    w_up,
    w_down,
    conv_in,
    c_gate,
    b_gate,
    conv_out,
    taps,
    w_out,
):
    sp_devices = lax.axis_size("sp")
    tok_rows = layer_grad.shape[0]
    top_count = routes.shape[1]
    capacity = expert_in.shape[1] // sp_devices
    full_grad = lax.all_gather(layer_grad, "tp", axis=1, tiled=True)
    flat_routes = routes.reshape(-1)
    onehot = (flat_routes[:, None] == jnp.arange(sp_devices, dtype=jnp.int32)[None, :]).astype(
        jnp.int32
    )
    slot_rank = jnp.sum((jnp.cumsum(onehot, axis=0) - 1) * onehot, axis=1)
    slot_index = flat_routes * capacity + slot_rank
    weights = route_weights[:, :, None]
    scaled = (weights * layer_grad[:, None, :].astype(jnp.float32)).astype(jnp.bfloat16)
    scaled = scaled.reshape(tok_rows * top_count, -1)
    buffer = (
        jnp.zeros((sp_devices * capacity, scaled.shape[1]), jnp.bfloat16).at[slot_index].set(scaled)
    )
    arrived = lax.all_to_all(
        buffer.reshape(sp_devices, capacity, -1), "sp", split_axis=0, concat_axis=0, tiled=True
    )
    expert_grad, saved_rows = (
        lax.all_gather(arrived.reshape(sp_devices * capacity, -1), "tp", axis=1, tiled=True),
        lax.all_gather(expert_in[0], "tp", axis=1, tiled=True),
    )
    gate_weight = w_gate[0]
    up_weight = w_up[0]
    down_weight = w_down[0]
    gate_pre = jnp.dot(saved_rows, gate_weight, preferred_element_type=jnp.float32)
    up_pre = jnp.dot(saved_rows, up_weight, preferred_element_type=jnp.float32)
    gate_cut = jnp.minimum(gate_pre, clamp_limit)
    up_cut = jnp.clip(up_pre, -clamp_limit, clamp_limit)
    sigmoid_gate = jax.nn.sigmoid(swish_alpha * gate_cut)
    hidden = ((up_cut + 1.0) * gate_cut * sigmoid_gate).astype(jnp.bfloat16)
    act_grad = jnp.einsum("rd,fd->rf", expert_grad, down_weight, preferred_element_type=jnp.float32)
    grad_down = jnp.einsum(
        "rf,rd->fd", hidden, expert_grad, preferred_element_type=jnp.float32
    ).astype(jnp.bfloat16)
    slope = sigmoid_gate + swish_alpha * gate_cut * sigmoid_gate * (1.0 - sigmoid_gate)
    gate_grad = jnp.where(gate_pre < clamp_limit, act_grad * (up_cut + 1.0) * slope, 0.0).astype(
        jnp.bfloat16
    )
    up_grad = jnp.where(
        jnp.abs(up_pre) < clamp_limit, act_grad * gate_cut * sigmoid_gate, 0.0
    ).astype(jnp.bfloat16)
    grad_gate = jnp.einsum(
        "rd,rf->df", saved_rows, gate_grad, preferred_element_type=jnp.float32
    ).astype(jnp.bfloat16)
    grad_up = jnp.einsum(
        "rd,rf->df", saved_rows, up_grad, preferred_element_type=jnp.float32
    ).astype(jnp.bfloat16)
    partial_value = jnp.einsum(
        "rf,df->rd", gate_grad, gate_weight, preferred_element_type=jnp.float32
    )
    partial_value = partial_value + jnp.einsum(
        "rf,df->rd", up_grad, up_weight, preferred_element_type=jnp.float32
    )
    rounded_terms = partial_value.astype(jnp.bfloat16)
    reduced = (
        lax.psum_scatter(rounded_terms, "tp", scatter_dimension=1, tiled=True)
        .astype(jnp.float32)
        .astype(jnp.bfloat16)
    )
    returned = lax.all_to_all(
        reduced.reshape(sp_devices, capacity, -1), "sp", split_axis=0, concat_axis=0, tiled=True
    )
    returned = returned.reshape(sp_devices * capacity, -1)
    picked = returned[slot_index]
    picked = picked.reshape(tok_rows, top_count, -1)
    grad_routed = jnp.sum(picked.astype(jnp.float32), axis=1).astype(jnp.bfloat16)
    mixer_grad = jnp.einsum("td,cd->tc", full_grad, w_out, preferred_element_type=jnp.float32)
    mixed = (b_gate.astype(jnp.float32) * conv_out.astype(jnp.float32)).astype(jnp.bfloat16)
    projected = lax.psum_scatter(
        jnp.einsum("td,tc->dc", full_grad, mixed, preferred_element_type=jnp.float32),
        "sp",
        scatter_dimension=0,
        tiled=True,
    )
    grad_out_proj = projected.T
    out_grad = mixer_grad * b_gate.astype(jnp.float32)
    tap_reach = taps.shape[0] - 1
    following = passed_along(out_grad[:tap_reach], "sp", -1)
    extended = jnp.concatenate([out_grad, following], axis=0)
    tap_values = taps.astype(jnp.float32)
    conv_grad = jnp.zeros_like(out_grad)
    for tap_index in range(tap_reach + 1):
        offset = tap_reach - tap_index
        conv_grad = conv_grad + tap_values[tap_index] * extended[offset : offset + tok_rows]
    grad_conv_in = (conv_grad * c_gate.astype(jnp.float32)).astype(jnp.bfloat16)
    grad_c_gate = (conv_grad * conv_in.astype(jnp.float32)).astype(jnp.bfloat16)
    grad_b_gate = (mixer_grad * conv_out.astype(jnp.float32)).astype(jnp.bfloat16)
    return (
        grad_gate[None],
        grad_up[None],
        grad_down[None],
        grad_routed,
        grad_out_proj,
        grad_conv_in,
        grad_c_gate,
        grad_b_gate,
    )


MESH = pl.DeviceIdType.MESH
bf16 = jnp.bfloat16
f32 = jnp.float32


def dot_nn(a, b):
    return jnp.dot(a, b, preferred_element_type=f32)


def dot_nt(a, b):
    return lax.dot_general(a, b, (((1,), (1,)), ((), ())), preferred_element_type=f32)


def dot_tn(a, b):
    return lax.dot_general(a, b, (((0,), (0,)), ((), ())), preferred_element_type=f32)


EXCHANGED = ("mirror",)
EARLY = "near"
EARLY_SIDES = (0,)
SWAP = 2
BACK = 2
FIRST_SAVED = ("own", "mirror", "beyond")


def fused_kernel(
    n_sp,
    lg_hbm,
    rt_hbm,
    wt_hbm,
    ein_hbm,
    wg_hbm,
    wu_hbm,
    wd_hbm,
    ci_hbm,
    cg_hbm,
    bg_hbm,
    co_hbm,
    taps_hbm,
    wo_hbm,
    gg_v,
    gu_v,
    gd_v,
    sel,
    ret,
    gop_ref,
    gci_ref,
    gcg_ref,
    gbg_ref,
    wg,
    wu,
    wd,
    wg_t,
    wu_t,
    wd_t,
    wo,
    fg,
    saved,
    saved_t,
    eg,
    disp,
    disp_far,
    row_scale,
    proj,
    proj_x,
    proj_xr,
    proj_n,
    proj_nr,
    proj_a,
    proj_ar,
    ext,
    halo,
    hid,
    hidden_t,
    fac_g,
    fac_u,
    ggrad,
    ugrad,
    terms,
    px,
    ysend,
    yrecv,
    red,
    rt_ref,
    wt_ref,
    ci_ref,
    cg_ref,
    bg_ref,
    co_ref,
    taps_ref,
    load_s,
    lg_s,
    lg_r,
    ein_s,
    ein_r,
    disp_s,
    disp_r,
    far_s,
    far_r,
    egs_s,
    egs_r,
    swap_s,
    swap_r,
    proj_s,
    proj_r,
    halo_s,
    halo_r,
    d2d_s,
    d2d_r,
    y_s,
    y_r,
    ret_s,
    ret_r,
):
    sp = lax.axis_index("sp")
    tp = lax.axis_index("tp")
    core, chip = lax.rem(tp, 2), lax.div(tp, 2)
    partner = chip * 2 + (1 - core)
    across = (1 - chip) * 2 + core
    plane, side = lax.div(sp, 2), lax.rem(sp, 2)
    planes = n_sp // 2
    sibling = plane * 2 + (1 - side)
    near = plane + 1 - 2 * lax.rem(plane, 2)
    mirror = lax.rem(plane + 2, planes)
    beyond = lax.rem(near + 2, planes)
    rows, dcols = ein_hbm.shape
    cap = rows // n_sp
    pair = 2 * cap
    width = fg.shape[1]
    tokens = fg.shape[0]
    top = rt_hbm.shape[0]
    quads = {"own": plane, "near": near, "mirror": mirror, "beyond": beyond}
    index = {"own": 0, "near": 1, "mirror": 2, "beyond": 3}

    def cols(j):
        return pl.ds(pl.multiple_of(j * dcols, dcols), dcols)

    def block(b):
        return pl.ds(pl.multiple_of(b * cap, cap), cap)

    def pair_rows(q):
        return pl.ds(pl.multiple_of(q * pair, pair), pair)

    mine, other = cols(tp), cols(across)
    corner = cols((1 - chip) * 2 + (1 - core))

    def load(src, dst, n):
        copy = pltpu.make_async_copy(src, dst, load_s.at[n])
        copy.start()
        return copy

    def remote(src, dst, send, recv, to_sp, to_tp):
        return pltpu.make_async_remote_copy(
            src_ref=src,
            dst_ref=dst,
            send_sem=send,
            recv_sem=recv,
            device_id=(to_sp, to_tp),
            device_id_type=MESH,
        )

    barrier = pltpu.get_barrier_semaphore()
    pl.semaphore_signal(barrier, inc=1, device_id=(sp, partner), device_id_type=MESH)
    pl.semaphore_signal(barrier, inc=1, device_id=(sp, across), device_id_type=MESH)
    for i in range(1, n_sp):
        pl.semaphore_signal(
            barrier, inc=1, device_id=(lax.rem(sp + i, n_sp), tp), device_id_type=MESH
        )
    lg_load = load(lg_hbm, fg.at[:, mine], 0)
    ein_load = load(ein_hbm, saved.at[:, mine], 1)
    route_load = load(rt_hbm, rt_ref, 6)
    weight_load = load(wt_hbm, wt_ref, 7)
    mixer_loads = [
        load(bg_hbm, bg_ref, 8),
        load(co_hbm, co_ref, 9),
        load(ci_hbm, ci_ref, 10),
        load(cg_hbm, cg_ref, 11),
        load(taps_hbm, taps_ref, 12),
    ]
    wo_load = load(wo_hbm, wo, 2)
    wg_load = load(wg_hbm, wg, 3)
    wu_load = load(wu_hbm, wu, 4)
    wd_load = load(wd_hbm, wd, 5)
    pl.semaphore_wait(barrier, n_sp + 1)

    def send(copy):
        copy.start()
        return copy

    def sent(region, sem):
        remote(region, region, sem, sem, sp, partner).wait_send()

    def await_region(region, s_sem, r_sem):
        remote(region, region, s_sem, r_sem, sp, partner).wait_recv()

    def saved_across(name, sides=(0, 1)):
        i = index[name]
        for x in sides:
            sl = block(quads[name] * 2 + x)
            region = saved.at[sl, mine]
            send(remote(region, region, ein_s, ein_r.at[i], sp, across))

    def saved_relay(name):
        region, i = saved.at[pair_rows(quads[name]), other], index[name]
        await_region(region, ein_s, ein_r.at[i])
        send(remote(region, region, ein_s, ein_r.at[5 + i], sp, partner))

    def saved_arrive(name):
        region = saved.at[pair_rows(quads[name]), corner]
        await_region(region, ein_s, ein_r.at[5 + index[name]])

    def homes(name, sides=(0, 1), order=SWAP):
        if name == "own":
            return [sibling]
        if order == 2:
            return [quads[name] * 2 + (1 - side) + x * (2 * side - 1) for x in sides]
        if order == 1:
            return [quads[name] * 2 + side + x * (1 - 2 * side) for x in sides]
        if order == 3:
            return [quads[name] * 2 + 1 - x for x in sides]
        return [quads[name] * 2 + x for x in sides]

    def rows_from(name):
        return block(sibling) if name == "own" else pair_rows(quads[name])

    lg_load.wait()
    lg_mine = fg.at[:, mine]
    send(remote(lg_mine, lg_mine, lg_s, lg_r.at[0], sp, across))
    send(remote(lg_mine, lg_mine, lg_s, lg_r.at[1], sp, partner))

    def saved_start():
        ein_load.wait()
        saved_across("mirror")
        saved_across(EARLY, EARLY_SIDES)
        region = saved.at[:, mine]
        send(remote(region, region, ein_s, ein_r.at[4], sp, partner))

    route_load.wait()
    weight_load.wait()
    expert_ids = lax.broadcasted_iota(jnp.int32, (n_sp, tokens), 0)
    named = jnp.zeros((n_sp, tokens), f32)
    weight = jnp.zeros((n_sp, tokens), f32)
    for k in range(top):
        hit = rt_ref[k : k + 1, :] == expert_ids
        named = jnp.where(hit, 1.0, named)
        weight = jnp.where(hit, wt_ref[k : k + 1, :], weight)
    earlier = (
        lax.broadcasted_iota(jnp.int32, (tokens, tokens), 0)
        < lax.broadcasted_iota(jnp.int32, (tokens, tokens), 1)
    )
    rank = dot_nn(named.astype(bf16), jnp.where(earlier, 1.0, 0.0).astype(bf16))
    rank = jnp.where(named > 0.0, rank, -1.0)
    slots = lax.broadcasted_iota(jnp.int32, (cap, tokens), 0).astype(f32)
    own_grad = fg[:, mine]
    for e in range(n_sp):
        chosen = slots == rank[e : e + 1, :]
        picks = jnp.where(chosen, 1.0, 0.0)
        row_weight = jnp.sum(jnp.where(chosen, weight[e : e + 1, :], 0.0), axis=1, keepdims=True)
        here = slice(e * cap, (e + 1) * cap)
        sel[here, :] = picks.astype(bf16)
        row_scale[here, :] = jnp.broadcast_to(row_weight, (cap, row_scale.shape[1]))
        disp[here, :] = (dot_nn(picks.astype(bf16), own_grad) * row_weight).astype(bf16)

    def dispatch(names):
        for name in names:
            for dest in homes(name):
                src, dst = disp.at[block(dest), :], eg.at[block(sp), mine]
                send(remote(src, dst, disp_s, disp_r.at[index[name]], dest, tp))

    def dispatch_far(names):
        for name in names:
            for dest in homes(name):
                src, dst = disp_far.at[block(dest), :], eg.at[block(sp), other]
                send(remote(src, dst, far_s, far_r.at[index[name]], dest, tp))

    def lg_relay():
        await_region(fg.at[:, other], lg_s, lg_r.at[0])
        send(remote(fg.at[:, other], fg.at[:, other], lg_s, lg_r.at[2], sp, partner))

    def select_across():
        far_grad = fg[:, other]
        for e in range(n_sp):
            here = slice(e * cap, (e + 1) * cap)
            disp_far[here, :] = (dot_nn(sel[here, :], far_grad) * row_scale[here, 0:1]).astype(bf16)

    def flip(src, dst):
        step = 512

        def part(j, carry):
            sl = pl.ds(pl.multiple_of(j * step, step), step)
            if src.shape[0] > src.shape[1]:
                dst[:, sl] = jnp.transpose(src[sl, :])
            else:
                dst[sl, :] = jnp.transpose(src[:, sl])
            return carry

        lax.fori_loop(0, width // step, part, 0)

    share = width // n_sp

    def mixer():
        wo_load.wait()
        for one in mixer_loads:
            one.wait()
        await_region(fg.at[:, cols(partner)], lg_s, lg_r.at[1])
        await_region(fg.at[:, corner], lg_s, lg_r.at[2])
        b_gate = bg_ref[...].astype(f32)
        conv_out = co_ref[...].astype(f32)
        mixer_grad = dot_nt(fg[...], wo[...])
        ext[0:tokens, :] = mixer_grad * b_gate
        gbg_ref[...] = (mixer_grad * conv_out).astype(bf16)
        before = lax.rem(sp + n_sp - 1, n_sp)
        halo_copy = send(remote(ext.at[0:8, :], halo, halo_s, halo_r, before, tp))
        mixed = (b_gate * conv_out).astype(bf16)
        for d in range(n_sp):
            proj[d % 2, d // 2] = dot_tn(mixed, fg[:, d * share : (d + 1) * share])
        proj_x[...] = proj[1 - side].astype(bf16)
        send(remote(proj_x, proj_xr, proj_s.at[0], proj_r.at[0], sibling, tp))
        return halo_copy

    def proj_near():
        await_region(proj_xr, proj_s.at[0], proj_r.at[0])
        for q in range(planes):
            proj[0, q] = proj[side, q] + proj_xr[q].astype(f32)
        proj_n[0] = proj[0, near].astype(bf16)
        proj_n[1] = proj[0, beyond].astype(bf16)
        send(remote(proj_n, proj_nr, proj_s.at[1], proj_r.at[1], near * 2 + side, tp))

    def proj_mirror():
        await_region(proj_nr, proj_s.at[1], proj_r.at[1])
        proj_a[...] = (proj[0, mirror] + proj_nr[1].astype(f32)).astype(bf16)
        send(remote(proj_a, proj_ar, proj_s.at[2], proj_r.at[2], mirror * 2 + side, tp))

    def proj_total():
        await_region(proj_ar, proj_s.at[2], proj_r.at[2])
        gop_ref[...] = proj[0, plane] + proj_nr[0].astype(f32) + proj_ar[...].astype(f32)

    def eg_mine(name):
        i, region = index[name], eg.at[pair_rows(quads[name]), mine]
        await_region(eg.at[rows_from(name), mine], disp_s, disp_r.at[i])
        if name in EXCHANGED:
            send(remote(region, region, swap_s, swap_r.at[EXCHANGED.index(name)], sp, across))
        send(remote(region, region, egs_s, egs_r.at[i], sp, partner))

    def eg_other(name):
        i, region = index[name], eg.at[pair_rows(quads[name]), other]
        if name in EXCHANGED:
            await_region(region, swap_s, swap_r.at[EXCHANGED.index(name)])
        else:
            await_region(eg.at[rows_from(name), other], far_s, far_r.at[i])
        send(remote(region, region, egs_s, egs_r.at[4 + i], sp, partner))

    def eg_arrive(name):
        sl, i = pair_rows(quads[name]), index[name]
        await_region(eg.at[sl, cols(partner)], egs_s, egs_r.at[i])
        await_region(eg.at[sl, corner], egs_s, egs_r.at[4 + i])

    def forward(name):
        sl = pair_rows(quads[name])
        x = saved[sl, :]
        gate_pre = dot_nn(x, wg[...])
        up_pre = dot_nn(x, wu[...])
        gate_cut = jnp.minimum(gate_pre, clamp_limit)
        up_cut = jnp.clip(up_pre, -clamp_limit, clamp_limit)
        sig = jax.nn.sigmoid(swish_alpha * gate_cut)
        base = gate_cut * sig
        slope = sig + swish_alpha * base * (1.0 - sig)
        hid[sl, :] = ((up_cut + 1.0) * base).astype(bf16)
        fac_g[sl, :] = jnp.where(gate_pre < clamp_limit, (up_cut + 1.0) * slope, 0.0)
        fac_u[sl, :] = jnp.where(jnp.abs(up_pre) < clamp_limit, base, 0.0)

    def backward(name):
        sl, i = pair_rows(quads[name]), index[name]
        act_grad = dot_nn(eg[sl, :], wd_t[...])
        g = (act_grad * fac_g[sl, :]).astype(bf16)
        u = (act_grad * fac_u[sl, :]).astype(bf16)
        ggrad[sl, :] = g
        ugrad[sl, :] = u

        def term(m):
            j = cols(m)
            terms[sl, j] = (dot_nn(g, wg_t[:, j]) + dot_nn(u, wu_t[:, j])).astype(bf16)

        for y in range(2):
            there = y * 2 + (1 - core)
            term(there)
            send(
                remote(
                    terms.at[sl, cols(there)],
                    px.at[sl, y * dcols : (y + 1) * dcols],
                    d2d_s,
                    d2d_r.at[i],
                    sp,
                    partner,
                )
            )
        for y in range(2):
            term(y * 2 + core)

    def pass_on(name, sides=(0, 1)):
        sl, i = pair_rows(quads[name]), index[name]
        if 0 in sides:
            await_region(px.at[sl, :], d2d_s, d2d_r.at[i])
        if len(sides) == 1:
            sl = block(quads[name] * 2 + sides[0])
        far = terms[sl, other].astype(f32) + px[sl, cols(1 - chip)].astype(f32)
        ysend[sl, :] = far.astype(bf16)
        send(remote(ysend.at[sl, :], yrecv.at[sl, :], y_s, y_r.at[i], sp, across))

    def add_up(name):
        sl, i = pair_rows(quads[name]), index[name]
        await_region(yrecv.at[sl, :], y_s, y_r.at[i])
        near_sum = terms[sl, mine].astype(f32) + px[sl, cols(chip)].astype(f32)
        red[sl, :] = (near_sum + yrecv[sl, :].astype(f32)).astype(bf16)
        if name == "own":
            ret[block(sp), :] = red[block(sp), :]

    def give(name, sides=(0, 1)):
        for dest in homes(name, sides, BACK):
            src, dst = red.at[block(dest), :], ret.at[block(sp), :]
            send(remote(src, dst, ret_s, ret_r.at[index[name]], dest, tp))

    def give_back(name):
        add_up(name)
        give(name)

    half = rows // 2

    def turn(h):
        part = pl.ds(pl.multiple_of(h * half, half), half)

        def step(j, carry):
            sl = pl.ds(pl.multiple_of(j * dcols, dcols), dcols)
            saved_t[sl, part] = jnp.transpose(saved[part, sl])
            return carry

        lax.fori_loop(0, width // dcols, step, 0)
        hidden_t[:, part] = jnp.transpose(hid[part, :])

    def down_tile(j, carry):
        sl = pl.ds(pl.multiple_of(j * dcols, dcols), dcols)
        gd_v[:, sl] = dot_nn(hidden_t[...], eg[:, sl]).astype(bf16)
        return carry

    tile = width // 8

    def weight_tile(j, carry):
        sl = pl.ds(pl.multiple_of(j * tile, tile), tile)
        x = saved_t[sl, :]
        gg_v[sl, :] = dot_nn(x, ggrad[...]).astype(bf16)
        gu_v[sl, :] = dot_nn(x, ugrad[...]).astype(bf16)
        return carry

    dispatch(("own", "mirror", "near", "beyond"))
    saved_start()
    eg[block(sp), mine] = disp[block(sp), :]
    wd_load.wait()
    flip(wd, wd_t)
    wg_load.wait()
    flip(wg, wg_t)
    wu_load.wait()
    flip(wu, wu_t)
    lg_relay()
    select_across()
    dispatch_far(("near", "own", "beyond"))
    eg[block(sp), other] = disp_far[block(sp), :]
    saved_relay("mirror")
    eg_mine("mirror")
    saved_across("near", (1,))
    saved_across("beyond")
    halo_copy = mixer()
    await_region(saved.at[:, cols(partner)], ein_s, ein_r.at[4])
    saved_arrive("mirror")
    forward("mirror")
    eg_other("mirror")
    eg_arrive("mirror")
    backward("mirror")
    proj_near()
    saved_relay("near")
    eg_mine("near")
    eg_other("near")
    pass_on("mirror")
    saved_across("own")
    saved_arrive("near")
    forward("near")
    saved_relay("beyond")
    eg_mine("own")
    eg_other("own")
    eg_mine("beyond")
    eg_arrive("near")
    backward("near")
    pass_on("near", (0,))
    proj_mirror()
    saved_arrive("beyond")
    forward("beyond")
    eg_other("beyond")
    give_back("mirror")
    eg_arrive("beyond")
    backward("beyond")
    pass_on("beyond")
    pass_on("near", (1,))
    saved_relay("own")
    turn(1 - lax.div(plane, 2))
    saved_arrive("own")
    forward("own")
    eg_arrive("own")
    backward("own")
    pass_on("own")
    give_back("beyond")
    turn(lax.div(plane, 2))
    give_back("near")
    halo_copy.wait_recv()
    ext[tokens : tokens + 8, :] = jnp.where(sp < n_sp - 1, halo[...], 0.0)
    reach = taps_ref.shape[0] - 1
    tap_values = taps_ref[...].astype(f32)
    conv_grad = tap_values[0:1, :] * ext[reach : reach + tokens, :]
    for j in range(1, reach + 1):
        conv_grad = conv_grad + tap_values[j : j + 1, :] * ext[reach - j : reach - j + tokens, :]
    gci_ref[...] = (conv_grad * cg_ref[...].astype(f32)).astype(bf16)
    gcg_ref[...] = (conv_grad * ci_ref[...].astype(f32)).astype(bf16)
    lax.fori_loop(0, width // dcols, down_tile, 0)
    lax.fori_loop(0, 1, weight_tile, 0)
    give_back("own")
    lax.fori_loop(1, 8, weight_tile, 0)
    proj_total()
    def await_back(name):
        await_region(ret.at[rows_from(name), :], ret_s, ret_r.at[index[name]])
    await_back("mirror")
    await_back("own")
    await_back("near")
    await_back("beyond")
    sent(fg.at[:, 0 : 3 * dcols], lg_s)
    sent(saved.at[:, 0 : 3 * dcols], ein_s)
    sent(disp.at[0 : (n_sp - 1) * cap, :], disp_s)
    sent(disp_far.at[0 : (n_sp - 1 - 2 * len(EXCHANGED)) * cap, :], far_s)
    sent(eg.at[:, 0 : 2 * dcols], egs_s)
    for _ in EXCHANGED:
        sent(eg.at[0:pair, 0:dcols], swap_s)
    sent(px, d2d_s)
    sent(ysend, y_s)
    sent(red.at[0 : (n_sp - 1) * cap, :], ret_s)
    sent(proj_x, proj_s.at[0])
    sent(proj_n, proj_s.at[1])
    sent(proj_a, proj_s.at[2])
    halo_copy.wait_send()


def write_out(*refs):
    gate, up, down, sel, ret = refs[:5]
    ready, outs, total, sems = (gate, up, down) + refs[5:9], refs[9:17], refs[17], refs[18]
    copies = []
    for n, (src, dst) in enumerate(zip(ready, outs[:3] + outs[4:])):
        copies.append(pltpu.make_async_copy(src, dst, sems.at[n]))
    for copy in copies:
        copy.start()
    total[...] = dot_tn(sel[...], ret[...]).astype(bf16)
    last = pltpu.make_async_copy(total, outs[3], sems.at[len(copies)])
    last.start()
    for copy in copies + [last]:
        copy.wait()


def fused(n_sp, layer_grad, routes, route_weights, expert_in, w_gate, w_up, w_down,
          conv_in, c_gate, b_gate, conv_out, taps, w_out):
    tokens, dcols = layer_grad.shape
    rows = expert_in.shape[1]
    width, units = w_gate.shape[1:]
    chans = conv_in.shape[1]
    share = width // n_sp
    planes = n_sp // 2
    any_spec = pl.BlockSpec(memory_space=pl.ANY)
    vmem = pl.BlockSpec(memory_space=pltpu.VMEM)
    dma = pltpu.SemaphoreType.DMA
    shape = jax.ShapeDtypeStruct
    kinds = (
        ((width, units), bf16),
        ((width, units), bf16),
        ((units, width), bf16),
        ((rows, tokens), bf16),
        ((rows, dcols), bf16),
        ((chans, share), f32),
        ((tokens, chans), bf16),
        ((tokens, chans), bf16),
        ((tokens, chans), bf16),
    )
    results = pl.pallas_call(
        functools.partial(fused_kernel, n_sp),
        out_shape=tuple(pltpu.VMEM(dims, dtype) for dims, dtype in kinds),
        in_specs=[any_spec] * 13,
        out_specs=(vmem,) * len(kinds),
        scratch_shapes=[
            pltpu.VMEM((width, units), bf16),
            pltpu.VMEM((width, units), bf16),
            pltpu.VMEM((units, width), bf16),
            pltpu.VMEM((units, width), bf16),
            pltpu.VMEM((units, width), bf16),
            pltpu.VMEM((width, units), bf16),
            pltpu.VMEM((chans, width), bf16),
            pltpu.VMEM((tokens, width), bf16),
            pltpu.VMEM((rows, width), bf16),
            pltpu.VMEM((width, rows), bf16),
            pltpu.VMEM((rows, width), bf16),
            pltpu.VMEM((rows, dcols), bf16),
            pltpu.VMEM((rows, dcols), bf16),
            pltpu.VMEM((rows, 128), f32),
            pltpu.VMEM((2, planes, chans, share), f32),
            pltpu.VMEM((planes, chans, share), bf16),
            pltpu.VMEM((planes, chans, share), bf16),
            pltpu.VMEM((2, chans, share), bf16),
            pltpu.VMEM((2, chans, share), bf16),
            pltpu.VMEM((chans, share), bf16),
            pltpu.VMEM((chans, share), bf16),
            pltpu.VMEM((tokens + 8, chans), f32),
            pltpu.VMEM((8, chans), f32),
            pltpu.VMEM((rows, units), bf16),
            pltpu.VMEM((units, rows), bf16),
            pltpu.VMEM((rows, units), f32),
            pltpu.VMEM((rows, units), f32),
            pltpu.VMEM((rows, units), bf16),
            pltpu.VMEM((rows, units), bf16),
            pltpu.VMEM((rows, width), bf16),
            pltpu.VMEM((rows, 2 * dcols), bf16),
            pltpu.VMEM((rows, dcols), bf16),
            pltpu.VMEM((rows, dcols), bf16),
            pltpu.VMEM((rows, dcols), bf16),
            pltpu.VMEM(routes.shape[::-1], jnp.int32),
            pltpu.VMEM(routes.shape[::-1], f32),
            pltpu.VMEM((tokens, chans), bf16),
            pltpu.VMEM((tokens, chans), bf16),
            pltpu.VMEM((tokens, chans), bf16),
            pltpu.VMEM((tokens, chans), bf16),
            pltpu.VMEM(taps.shape, bf16),
            dma((13,)),
            dma,
            dma((3,)),
            dma,
            dma((9,)),
            dma,
            dma((4,)),
            dma,
            dma((4,)),
            dma,
            dma((8,)),
            dma,
            dma((2,)),
            dma((3,)),
            dma((3,)),
            dma,
            dma,
            dma,
            dma((4,)),
            dma,
            dma((4,)),
            dma,
            dma((4,)),
        ],
        compiler_params=pltpu.CompilerParams(
            collective_id=0, has_side_effects=True, vmem_limit_bytes=52 * 1024 * 1024
        ),
    )(
        layer_grad,
        routes.T,
        route_weights.T,
        expert_in[0],
        w_gate[0],
        w_up[0],
        w_down[0],
        conv_in,
        c_gate,
        b_gate,
        conv_out,
        taps,
        w_out,
    )
    results = pl.pallas_call(
        write_out,
        out_shape=tuple(
            shape(dims, dtype)
            for dims, dtype in kinds[:3] + (((tokens, dcols), bf16),) + kinds[5:]
        ),
        in_specs=[vmem] * len(kinds),
        out_specs=(any_spec,) * (len(kinds) - 1),
        scratch_shapes=[pltpu.VMEM((tokens, dcols), bf16), dma((len(kinds) - 1,))],
        compiler_params=pltpu.CompilerParams(vmem_limit_bytes=2 * 1024 * 1024),
    )(*results)
    gate, up, down = results[:3]
    return (gate[None], up[None], down[None]) + tuple(results[3:])


def dispatching(n_sp, n_tp, layer_grad, routes, route_weights, expert_in, *others):
    tokens, dcols = layer_grad.shape
    cap = expert_in.shape[1] // n_sp
    chans = others[3].shape[1]
    fits = (
        n_tp == 4
        and n_sp == 8
        and cap % 16 == 0
        and tokens % 128 == 0
        and dcols % 128 == 0
        and chans % 128 == 0
        and (dcols * n_tp) % (n_sp * 128) == 0
        and others[-2].shape[0] <= 9
    )
    if fits:
        return fused(n_sp, layer_grad, routes, route_weights, expert_in, *others)
    return per_device(layer_grad, routes, route_weights, expert_in, *others)


def solution(mesh):
    in_specs = (
        P("sp", "tp"),
        P("sp", None),
        P("sp", None),
        P("sp", None, "tp"),
        P("sp", None, "tp"),
        P("sp", None, "tp"),
        P("sp", "tp", None),
        P("sp", "tp"),
        P("sp", "tp"),
        P("sp", "tp"),
        P("sp", "tp"),
        P(None, "tp"),
        P("tp", None),
    )
    out_specs = (
        P("sp", None, "tp"),
        P("sp", None, "tp"),
        P("sp", "tp", None),
        P("sp", "tp"),
        P("tp", "sp"),
        P("sp", "tp"),
        P("sp", "tp"),
        P("sp", "tp"),
    )
    return jax.shard_map(
        functools.partial(dispatching, mesh.shape["sp"], mesh.shape["tp"]), mesh=mesh, in_specs=in_specs, out_specs=out_specs, check_vma=False
    )
```
